32 devices in a mesh: grp: 2 (over y), sp: 4 (over z), tp: 4 (over x, core).
Axes of the slice: x: 2, y: 2, z: 4, core: 2. Of those that a mesh axis runs over, the one named last changes fastest.
Arguments:
- tokens: bfloat16 [8, 1024, 4096], P(('grp', 'tp'), 'sp'), parts along dimension 0, may hold values from -8 to 8, as said below
- offsets: int32 [8], P(('grp', 'tp')), parts along dimension 0, may hold values from 0 to 4095
- in_gain: float32 [4096], replicated, may hold values from 0.1 to 1.9
- w_latent: bfloat16 [4096, 1024], P('sp'), may hold values from -0.09375 to 0.09375
- w_rope_key: bfloat16 [4096, 32], replicated, may hold values from -0.09375 to 0.09375
- kv_gain: float32 [1024], replicated, may hold values from 0.1 to 1.9
- w_up_key: bfloat16 [1024, 2048], P(None, 'tp'), may hold values from -0.1875 to 0.1875
- w_up_value: bfloat16 [1024, 2048], P(None, 'tp'), may hold values from -0.1875 to 0.1875
- q_nope: bfloat16 [8, 2048], P(('grp', 'sp'), 'tp'), parts along dimension 0, may hold values from -300 to 300, as said below
- q_rope: bfloat16 [8, 1024], P(('grp', 'sp'), 'tp'), parts along dimension 0, may hold values from -16 to 16
Outputs:
- keys: bfloat16 [8, 1024, 2048], P(('grp', 'sp'), None, 'tp'), parts along dimension 0
- values: bfloat16 [8, 1024, 2048], P(('grp', 'sp'), None, 'tp'), parts along dimension 0
- rope_keys: bfloat16 [8, 32, 1024], P(('grp', 'sp')), parts along dimension 0
- read: bfloat16 [8, 2048], P(('grp', 'sp'), 'tp'), parts along dimension 0
The draws below stay inside these ranges and needn't reach their ends.
There are 2 independent parts, one for each index of `grp`. The reference program is written for one: setup_inputs(seed, part) draws one part's arguments, and reference() takes and returns one part's arrays. A program takes and returns all parts, laid end to end along the dimension named above; an argument that names none is the same for every part. Nothing has to cross between parts.
Inputs may be any that keep to these rules, and one draw needn't show every extreme that they name: `tokens`: entries of the layer's input. `q_nope`: entries of the first decoding token's queries.
All inputs are finite; a program needn't handle non-finite values.
Results may differ from the reference program's by a relative error of at most 0.02.
Values may be sent and summed in bfloat16 or wider, within the bound.
A program may use at most 128 MiB of HBM per device.

```python
import jax
import jax.numpy as jnp
from jax import lax

D = 4096
HEADS = 32
HEAD = 64
ROPE = 32
KV_RANK = 1024
SEQS = 4
LEN = 1024


def draw_tokens(key, part):
    first, second = jax.random.split(jax.random.fold_in(key, 29))
    noise = jax.random.normal(first, (SEQS, LEN, D), jnp.float32)
    base = jnp.clip(noise, -6.0, 6.0)
    return base.astype(jnp.bfloat16)


def draw_q_nope(key, part):
    first, second = jax.random.split(jax.random.fold_in(key, 17))
    base = jax.random.normal(first, (SEQS, HEADS, HEAD), jnp.float32) * 4.0
    base = jnp.clip(base, -16.0, 16.0)
    return base.reshape(SEQS, HEADS * HEAD).astype(jnp.bfloat16)


def plant(array, key, low, largest):
    place = [jax.random.randint(jax.random.fold_in(key, axis), (), 0, length) for axis, length in enumerate(array.shape)]
    widest = array.shape.index(max(array.shape))
    neighbour = place[:widest] + [(place[widest] + 1) % array.shape[widest]] + place[widest + 1:]
    return array.at[tuple(place)].set(low).at[tuple(neighbour)].set(largest)


def block_levels(stream_key, extent, pieces, low, top_value):
    loudness = 1.0
    for dim, parts in pieces:
        steps = jax.random.uniform(jax.random.fold_in(jax.random.fold_in(stream_key, 6), dim), (parts,), jnp.float32, low / len(pieces), top_value / len(pieces))
        loudness = loudness * jnp.repeat(jnp.exp(steps), extent[dim] // parts).reshape((-1,) + (1,) * (len(extent) - 1 - dim))
    return loudness


def normal_values(key, extent, deviation, reach, shards=(), kind=jnp.bfloat16):
    drawn = deviation * jax.random.normal(key, extent, jnp.float32)
    if shards:
        drawn = drawn * block_levels(key, extent, shards, -0.22, 0.18)
    return jnp.clip(drawn, -reach, reach).astype(kind)


def setup_inputs(seed: int = 0, part: int = 0) -> dict:
    key_list = jax.random.split(jax.random.key(seed), 11)
    own_keys = jax.random.split(jax.random.fold_in(key_list[10], part), 11)
    return {
        "tokens": draw_tokens(jax.random.fold_in(jax.random.fold_in(key_list[10], part), 71), part),
        "offsets": plant(jax.random.randint(own_keys[1], (SEQS,), 0, 4096), jax.random.fold_in(own_keys[1], 1), 0, 4095).astype(jnp.int32),
        "in_gain": jnp.clip(1.0 + 0.18 * jax.random.normal(key_list[2], (D,), jnp.float32), 0.1, 1.9),
        "w_latent": normal_values(key_list[3], (D, KV_RANK), D ** -0.5, 0.09375, ((0, 4),)),
        "w_rope_key": normal_values(key_list[4], (D, ROPE), D ** -0.5, 0.09375),
        "kv_gain": jnp.clip(1.0 + 0.18 * jax.random.normal(key_list[5], (KV_RANK,), jnp.float32), 0.1, 1.9),
        "w_up_key": normal_values(key_list[6], (KV_RANK, HEADS * HEAD), KV_RANK ** -0.5, 0.1875, ((1, 4),)),
        "w_up_value": normal_values(key_list[7], (KV_RANK, HEADS * HEAD), KV_RANK ** -0.5, 0.1875, ((1, 4),)),
        "q_nope": draw_q_nope(jax.random.fold_in(jax.random.fold_in(key_list[10], part), 71), part),
        "q_rope": normal_values(own_keys[9], (SEQS, HEADS * ROPE), 4.0, 16.0, ((0, 4), (1, 4))),
    }


EPS = 1e-06

def rms_scale(values, gain):
    wide = values.astype(jnp.float32)
    return wide * lax.rsqrt(lax.optimization_barrier(jnp.mean(wide * wide, axis=-1, keepdims=True)) + EPS) * gain.astype(jnp.float32)

def rotate(raw, position):
    inverse = 10000.0 ** (-jnp.arange(0, ROPE, 2).astype(jnp.float32) / ROPE)
    angle = position.astype(jnp.float32)[:, None] * inverse[None, :]
    cosine, sine = (jnp.cos(angle), jnp.sin(angle))
    half = ROPE // 2
    first, second = (raw[:, :half], raw[:, half:])
    return jnp.concatenate([first * cosine - second * sine, second * cosine + first * sine], axis=-1)

def reference(tokens, offsets, in_gain, w_latent, w_rope_key, kv_gain, w_up_key, w_up_value, q_nope, q_rope):

    def one_prompt(args):
        prompt, start = args
        normed = rms_scale(prompt, in_gain).astype(jnp.bfloat16)
        latent_raw = jnp.dot(normed, w_latent, preferred_element_type=jnp.float32)
        latent = rms_scale(latent_raw, kv_gain).astype(jnp.bfloat16)
        rope_raw = jnp.dot(normed, w_rope_key, preferred_element_type=jnp.float32)
        position = start + jnp.arange(LEN, dtype=jnp.int32)
        rotated = rotate(rope_raw, position).astype(jnp.bfloat16)
        keys = jnp.dot(latent, w_up_key, preferred_element_type=jnp.float32).astype(jnp.bfloat16)
        values = jnp.dot(latent, w_up_value, preferred_element_type=jnp.float32).astype(jnp.bfloat16)
        return (keys, values, rotated.T)
    keys, values, rope_keys = lax.map(one_prompt, (tokens, offsets))
    query = q_nope.astype(jnp.float32).reshape(SEQS, HEADS, HEAD)
    rotary_q = q_rope.astype(jnp.float32).reshape(SEQS, HEADS, ROPE)
    keys_wide = keys.astype(jnp.float32).reshape(SEQS, LEN, HEADS, HEAD)
    scores = jnp.einsum('shd,sjhd->shj', query, keys_wide)
    scores = scores + jnp.einsum('shr,srj->shj', rotary_q, rope_keys.astype(jnp.float32))
    scores = scores / jnp.sqrt(jnp.float32(HEAD + ROPE))
    weights = jax.nn.softmax(scores, axis=-1).astype(jnp.bfloat16)
    values_wide = values.astype(jnp.float32).reshape(SEQS, LEN, HEADS, HEAD)
    read = jnp.einsum('shj,sjhd->shd', weights.astype(jnp.float32), values_wide)
    read = read.astype(jnp.bfloat16).reshape(SEQS, HEADS * HEAD)
    return (keys, values, rope_keys, read)
```

```python
import functools

import jax
import jax.numpy as jnp
import numpy as np
from jax import lax
from jax.experimental import pallas as pl
from jax.experimental.pallas import tpu as pltpu
from jax.sharding import PartitionSpec as P

HEAD = 64
ROPE = 32
CORES = 2
PIECES = 4
PENDING = 60
PARTS = (1, 1, 1, 1, 1, 1, 1, 1)
MODES = ("F", "O", "F", "O", "F", "O", "C", "O", "F")
X_FIRST = (True, True, True, True, False, True, False, True, True, True, True, True, True, True, False, True, True, True, True, False, True, True, True, True)
OUTER = (
    ("own", 0), ("own", 1), ("own", 2), ("norm", 1), ("norm", 0), ("a", 0), ("norm", 2), ("a", 3),
    ("own", 3), ("norm", 3), ("odot", 0), ("odot", 5), ("b", 0), ("odot", 3), ("odot", 2),
    ("odot", 4), ("a", 1), ("odot", 6), ("odot", 7), ("own", 4), ("odot", 1), ("a", 9), ("b", 3),
    ("a", 6), ("a", 4), ("b", 1), ("a", 7), ("own", 5), ("a", 2), ("l", 0), ("b", 9), ("c", 3),
    ("b", 6), ("t", 0), ("b", 7), ("a", 10), ("a", 12), ("b", 4), ("c", 0), ("dot", 0), ("b", 2),
    ("c", 9), ("own", 6), ("c", 6), ("a", 5), ("a", 8), ("b", 10), ("c", 1), ("a", 11), ("dot", 6),
    ("d", 0, 0), ("d", 0, 2), ("d", 0, 3), ("d", 0, 1), ("a", 15), ("b", 12), ("dot", 3), ("c", 7),
    ("c", 4), ("dot", 1), ("a", 18), ("b", 8), ("a", 13), ("c", 2), ("a", 16), ("own", 7),
    ("dot", 7), ("dot", 4), ("a", 14), ("b", 5), ("b", 16), ("b", 13), ("b", 11), ("b", 15),
    ("dot", 2), ("l", 1), ("a", 17), ("a", 21), ("c", 12), ("a", 19), ("c", 10), ("b", 18),
    ("a", 20), ("dot", 10), ("b", 21), ("d", 1, 2), ("dot", 12), ("a", 22), ("b", 20), ("c", 8),
    ("c", 13), ("b", 17), ("c", 5), ("b", 14), ("dot", 9), ("a", 23), ("dot", 8), ("l", 3),
    ("dot", 5), ("l", 2), ("c", 11), ("b", 22), ("b", 23), ("c", 14), ("c", 15), ("d", 1, 3),
    ("dot", 13), ("dot", 11), ("l", 4), ("b", 19), ("d", 1, 1), ("t", 2), ("d", 1, 0), ("dot", 14),
    ("l", 5), ("d", 5, 1), ("dot", 15), ("c", 16), ("d", 2, 0), ("c", 18), ("d", 2, 2), ("c", 17),
    ("t", 4), ("e", 1, 3), ("dot", 18), ("c", 20), ("c", 19), ("dot", 16), ("e", 1, 2), ("d", 2, 3),
    ("d", 2, 1), ("dot", 19), ("d", 3, 2), ("dot", 17), ("l", 6), ("c", 21), ("d", 4, 2),
    ("d", 4, 1), ("dot", 21), ("d", 4, 0), ("e", 1, 1), ("dot", 20), ("l", 7), ("d", 3, 1),
    ("d", 5, 3), ("d", 3, 3), ("d", 4, 3), ("d", 5, 2), ("t", 6), ("c", 22), ("c", 23), ("d", 6, 2),
    ("dot", 22), ("d", 3, 0), ("dot", 23), ("l", 8), ("d", 6, 0), ("e", 5, 1), ("d", 7, 1),
    ("e", 3, 1), ("d", 6, 3), ("d", 6, 1), ("d", 7, 2), ("e", 5, 2), ("e", 5, 3), ("e", 3, 2),
    ("e", 6, 2), ("d", 7, 0), ("d", 7, 3), ("e", 7, 1), ("t", 8), ("e", 6, 1), ("e", 6, 3),
    ("d", 8, 1), ("d", 5, 0), ("e", 3, 3), ("e", 7, 2), ("e", 7, 3), ("d", 8, 0), ("d", 8, 2),
    ("d", 8, 3), ("end", 0, 0), ("end", 0, 1), ("end", 0, 2), ("end", 0, 3), ("end", 1, 0),
    ("end", 1, 1), ("end", 1, 2), ("end", 1, 3), ("end", 2, 0), ("end", 2, 1), ("end", 2, 2),
    ("end", 2, 3), ("end", 3, 0), ("end", 3, 1), ("end", 3, 2), ("end", 3, 3), ("end", 4, 0),
    ("end", 4, 1), ("end", 4, 2), ("end", 4, 3), ("end", 5, 0), ("end", 5, 1), ("end", 5, 2),
    ("end", 5, 3), ("end", 6, 0), ("end", 6, 1), ("end", 6, 2), ("end", 6, 3), ("end", 7, 0),
    ("end", 7, 1), ("end", 7, 2), ("end", 7, 3), ("end", 8, 0), ("end", 8, 1), ("end", 8, 2),
    ("end", 8, 3),
)
MIDDLE = (
    ("own", 0), ("own", 1), ("norm", 1), ("own", 2), ("norm", 0), ("norm", 2), ("z", 0), ("a", 0),
    ("z", 1), ("a", 1), ("own", 3), ("z", 4), ("a", 4), ("norm", 3), ("odot", 1), ("odot", 3),
    ("z", 7), ("a", 7), ("odot", 2), ("odot", 4), ("z", 2), ("a", 2), ("odot", 6), ("b", 1),
    ("z", 6), ("a", 6), ("z", 3), ("z", 9), ("a", 9), ("a", 3), ("odot", 0), ("z", 10), ("b", 4),
    ("odot", 7), ("l", 0), ("own", 4), ("a", 10), ("b", 0), ("c", 1), ("z", 5), ("a", 5), ("z", 8),
    ("a", 8), ("b", 7), ("b", 6), ("b", 3), ("z", 12), ("a", 12), ("z", 13), ("own", 5), ("t", 0),
    ("a", 13), ("z", 11), ("a", 11), ("b", 9), ("b", 2), ("odot", 5), ("z", 15), ("a", 15),
    ("c", 4), ("c", 0), ("dot", 0), ("c", 7), ("d", 0, 1), ("b", 10), ("z", 16), ("a", 16),
    ("dot", 1), ("own", 6), ("z", 14), ("a", 14), ("c", 6), ("b", 5), ("b", 8), ("z", 17),
    ("dot", 4), ("z", 19), ("own", 7), ("b", 12), ("c", 3), ("c", 2), ("d", 0, 0), ("b", 11),
    ("d", 0, 2), ("z", 18), ("a", 18), ("dot", 3), ("b", 13), ("a", 17), ("a", 19), ("dot", 6),
    ("c", 9), ("dot", 2), ("l", 1), ("b", 14), ("c", 10), ("b", 16), ("z", 21), ("a", 21),
    ("b", 15), ("z", 20), ("a", 20), ("b", 17), ("z", 22), ("a", 22), ("c", 5), ("c", 8), ("z", 23),
    ("a", 23), ("b", 18), ("dot", 7), ("dot", 5), ("l", 2), ("dot", 8), ("l", 3), ("d", 0, 3),
    ("c", 11), ("d", 1, 2), ("b", 20), ("dot", 9), ("c", 14), ("dot", 10), ("b", 19), ("dot", 14),
    ("b", 22), ("c", 12), ("d", 1, 1), ("d", 1, 0), ("dot", 11), ("l", 4), ("c", 13), ("b", 23),
    ("d", 1, 3), ("b", 21), ("dot", 13), ("d", 3, 2), ("dot", 12), ("l", 5), ("t", 2), ("c", 19),
    ("c", 16), ("c", 15), ("dot", 15), ("t", 4), ("d", 4, 0), ("c", 17), ("dot", 17), ("d", 3, 1),
    ("d", 3, 0), ("c", 18), ("dot", 19), ("e", 1, 2), ("d", 5, 2), ("d", 3, 3), ("c", 20),
    ("d", 2, 0), ("dot", 16), ("l", 6), ("d", 4, 2), ("dot", 18), ("e", 3, 1), ("d", 5, 0),
    ("e", 1, 1), ("t", 6), ("dot", 20), ("l", 7), ("d", 4, 1), ("c", 22), ("dot", 22), ("d", 4, 3),
    ("c", 21), ("c", 23), ("d", 5, 1), ("dot", 21), ("d", 2, 2), ("d", 5, 3), ("dot", 23), ("l", 8),
    ("d", 7, 2), ("e", 1, 3), ("d", 2, 1), ("e", 3, 2), ("d", 2, 3), ("d", 6, 2), ("d", 7, 1),
    ("d", 7, 3), ("t", 8), ("e", 5, 1), ("e", 5, 3), ("d", 6, 1), ("e", 3, 3), ("e", 5, 2),
    ("d", 6, 0), ("d", 7, 0), ("e", 7, 2), ("d", 6, 3), ("e", 6, 1), ("e", 6, 2), ("e", 7, 3),
    ("e", 6, 3), ("d", 8, 1), ("d", 8, 0), ("e", 7, 1), ("d", 8, 3), ("d", 8, 2), ("end", 0, 0),
    ("end", 0, 1), ("end", 0, 2), ("end", 0, 3), ("end", 1, 0), ("end", 1, 1), ("end", 1, 2),
    ("end", 1, 3), ("end", 2, 0), ("end", 2, 1), ("end", 2, 2), ("end", 2, 3), ("end", 3, 0),
    ("end", 3, 1), ("end", 3, 2), ("end", 3, 3), ("end", 4, 0), ("end", 4, 1), ("end", 4, 2),
    ("end", 4, 3), ("end", 5, 0), ("end", 5, 1), ("end", 5, 2), ("end", 5, 3), ("end", 6, 0),
    ("end", 6, 1), ("end", 6, 2), ("end", 6, 3), ("end", 7, 0), ("end", 7, 1), ("end", 7, 2),
    ("end", 7, 3), ("end", 8, 0), ("end", 8, 1), ("end", 8, 2), ("end", 8, 3),
)

EPS = 1e-06
MESH = pl.DeviceIdType.MESH


def column_groups(n_sp, cols):
    if n_sp > 4 or cols % 1024:
        return [(0, cols)]
    each, total, out = cols // sum(PARTS), 0, []
    for part in PARTS:
        out.append((total, part * each))
        total += part * each
    return out


def plain_schedule(units, groups, n_sp):
    late = len(units) * 10
    ops = [(g, ("own", g)) for g in range(groups)]
    ops += [(k, ("norm", k)) for k in range(PIECES)]
    ops += [(PIECES + g, ("odot", g)) for g in range(groups)]
    done = {}
    for u, (g, d) in enumerate(units):
        at = PIECES + 2 + u
        ops += [(at, ("a", u)), (at + 2, ("b", u)), (at + 4, ("c", u)), (at + 5, ("dot", u))]
        done[g + 1] = at + 5
    for m in range(groups + 1):
        at = done.get(m, PIECES + 1)
        ops += [(at + 0.5, ("l", m)), (at + 3, ("t", m))]
        ops += [(at + 6, ("d", m, d)) for d in range(n_sp)]
        ops += [(late + m, ("end", m, d)) for d in range(n_sp)]
    return [op for _, op in sorted(ops, key=lambda item: item[0])]


def gather_kernel(n_grp, n_sp, n_tp, spans, frequency, *refs):
    groups = len(spans)
    tok_hbm, w_hbm, w_rope_hbm, gain_hbm, offsets, lat_out, rope_out = refs[:7]
    tok, w_own, w_rope, in_gain, normed = refs[7:12]
    wbuf, acc, own, transit = (refs[12 + k * groups : 12 + (k + 1) * groups] for k in range(4))
    (
        own_rope,
        transit_rope,
        local_sem,
        own_send,
        z_send,
        z_recv,
        a_send,
        a_recv,
        b_send,
        b_recv,
        c_send,
        c_recv,
        l_send,
        t_send,
        t_recv,
        x_send,
        e_send,
        d_send,
        l_recv,
    ) = refs[12 + 4 * groups :]
    n_x = n_tp // CORES
    prompts, rows = own[0].shape[:2]
    depth, cols = w_own.shape
    chunk = depth // (n_grp * n_tp)
    y, z, t = lax.axis_index("grp"), lax.axis_index("sp"), lax.axis_index("tp")
    x, core = t // CORES, t % CORES
    rank = (core * n_x + x) * n_grp + y

    def tp_of(x_to, core_to):
        return {"tp": x_to * CORES + core_to}

    partner = tp_of(x, 1 - core)
    x_peers = [lax.rem(x + k, n_x) for k in range(1, n_x)]
    y_peers = [lax.rem(y + k, n_grp) for k in range(1, n_grp)]
    z_up, z_down = lax.rem(z + 1, n_sp), lax.rem(z + n_sp - 1, n_sp)
    has_up, has_down = z + 1 < n_sp, z > 0

    fetch_tok = pltpu.make_async_copy(tok_hbm, tok, local_sem.at[0])
    fetch_w = pltpu.make_async_copy(w_hbm, w_own, local_sem.at[1])
    fetch_rope = pltpu.make_async_copy(w_rope_hbm, w_rope, local_sem.at[2])
    fetch_gain = pltpu.make_async_copy(gain_hbm, in_gain, local_sem.at[3])

    barrier = pltpu.get_barrier_semaphore()

    def greet(target):
        pl.semaphore_signal(barrier, inc=1, device_id=target, device_id_type=MESH)

    pl.when(has_up)(lambda: greet({"sp": z_up}))
    pl.when(has_down)(lambda: greet({"sp": z_down}))
    near = [tp_of(p, core) for p in x_peers] + [{"grp": p} for p in y_peers] + [partner]
    for target in near:
        greet(target)
    fetch_gain.start()
    fetch_tok.start()
    fetch_w.start()
    fetch_rope.start()
    pl.semaphore_wait(barrier, len(near) + has_up.astype(jnp.int32) + has_down.astype(jnp.int32))

    finish, fetched = [], []
    tuned = n_sp == 4 and groups == len(PARTS)
    modes = MODES if tuned else ("F",) * (groups + 1)

    def remote(src, dst, send, recv, device):
        return pltpu.make_async_remote_copy(
            src_ref=src,
            dst_ref=dst,
            send_sem=send,
            recv_sem=recv,
            device_id=device,
            device_id_type=MESH,
        )

    def arrived(ref, recv):
        remote(ref, ref, recv, recv, partner).wait_recv()

    def need(copy):
        if not any(copy is other for other in fetched):
            fetched.append(copy)
            copy.wait()

    def begin(copy, when=None):
        if when is None:
            copy.start()
            finish.append(copy.wait_send)
        else:
            pl.when(when)(copy.start)
            finish.append(lambda: pl.when(when)(copy.wait_send))

    units = [(g, d) for g in range(groups) for d in range(1, n_sp)]
    above = n_sp - 1 - z
    both = jnp.minimum(z, above)

    def shard(d):
        paired = d <= 2 * both
        hop = jnp.where(paired, (d + 1) // 2, d - both)
        up = jnp.where(paired, d % 2 == 1, above > z)
        return jnp.where(up, z + hop, z - hop), up

    shards = {d: shard(d) for d in range(1, n_sp)}

    def own_z(g):
        first, width = spans[g]
        for side, ahead, exists in ((0, z_up, has_up), (1, z_down, has_down)):
            copy = remote(
                w_hbm.at[pl.ds(rank * chunk, chunk), pl.ds(first, width)],
                wbuf[g].at[z, core, x, y],
                own_send.at[g, side],
                z_recv.at[g, z],
                {"sp": ahead},
            )
            begin(copy, exists)

    def x_first(u):
        return X_FIRST[u] if tuned else u % 4 > 0

    def spread(u, src, send, recv, along_x):
        peers = x_peers if along_x else y_peers
        for k, peer in enumerate(peers):
            device = tp_of(peer, core) if along_x else {"grp": peer}
            begin(remote(src, src, send.at[u, k], recv.at[u, k], device))

    def block_a(u):
        g, d = units[u]
        return wbuf[g].at[shards[d][0], core, x, y]

    def block_b(u):
        g, d = units[u]
        if x_first(u):
            return wbuf[g].at[shards[d][0], core, :, y]
        return wbuf[g].at[shards[d][0], core, x]

    def stage_z(u):
        g, d = units[u]
        s, up = shards[d]
        arrived(block_a(u), z_recv.at[g, s])
        exists = jnp.where(up, has_down, has_up)
        ahead = jnp.where(up, z_down, z_up)
        begin(
            remote(block_a(u), block_a(u), z_send.at[u], z_recv.at[g, s], {"sp": ahead}), exists
        )

    def stage_a(u):
        spread(u, block_a(u), a_send, a_recv, x_first(u))

    def stage_b(u):
        for k in range(len(x_peers if x_first(u) else y_peers)):
            arrived(block_a(u), a_recv.at[u, k])
        spread(u, block_b(u), b_send, b_recv, not x_first(u))

    def stage_c(u):
        g, d = units[u]
        for k in range(len(y_peers if x_first(u) else x_peers)):
            arrived(block_b(u), b_recv.at[u, k])
        ref = wbuf[g].at[shards[d][0], core]
        begin(remote(ref, ref, c_send.at[u], c_recv.at[u], partner))

    def stage_dot(u):
        g, d = units[u]
        s, _ = shards[d]
        arrived(wbuf[g].at[s, core], c_recv.at[u])
        weight = wbuf[g][s].reshape(depth, spans[g][1])
        acc[g][...] += jnp.dot(normed[s], weight, preferred_element_type=jnp.float32)

    def slot(m, s):
        if m == 0:
            return rope_out.at[s]
        first, width = spans[m - 1]
        return lat_out.at[s, :, pl.ds(first, width)]

    def mine(m, i):
        return own_rope.at[i] if m == 0 else own[m - 1].at[i]

    def held(m, k, i):
        return transit_rope.at[k, i] if m == 0 else transit[m - 1].at[k, i]

    def stage_l(m):
        for i in range(prompts):
            home = t * prompts + i
            if modes[m] != "C":
                copy = remote(
                    mine(m, i), slot(m, z), l_send.at[m, i], l_recv.at[m, z], {"sp": home}
                )
                begin(copy, home != z)
            for k, peer in enumerate(x_peers):
                device = tp_of(peer, core)
                beside = remote(mine(m, i), slot(m, z), x_send.at[m, i, k], l_recv.at[m, z], device)
                begin(beside, home == z)
                if modes[m] == "D":
                    routed = remote(
                        mine(m, i),
                        slot(m, z),
                        x_send.at[m, i, k],
                        l_recv.at[m, z],
                        device | {"sp": home},
                    )
                    begin(routed, home != z)
                elif modes[m] != "O":
                    across = remote(
                        mine(m, i), held(m, k, i), x_send.at[m, i, k], t_recv.at[m, k, i], device
                    )
                    begin(across, home != z)

    def stage_t(m):
        if modes[m] not in "FC":
            return
        for k in range(n_x - 1):
            source = lax.rem(x + n_x - 1 - k, n_x) * CORES + core
            for i in range(prompts):
                home = source * prompts + i
                copy = remote(
                    held(m, k, i), slot(m, z), t_send.at[m, k, i], l_recv.at[m, z], {"sp": home}
                )

                def pass_on(k=k, i=i, copy=copy):
                    arrived(held(m, k, i), t_recv.at[m, k, i])
                    copy.start()

                pl.when(home != z)(pass_on)
                finish.append(lambda home=home, copy=copy: pl.when(home != z)(copy.wait_send))

    owner = z // prompts
    x_in, core_in = owner // CORES, owner % CORES

    def partner_copy(m, d, s):
        return remote(slot(m, s), slot(m, s), d_send.at[m, d], l_recv.at[m, s], partner)

    def enters(m, d):
        here = core == core_in
        if d == 0 or modes[m] in "FD":
            return here
        return here & ((x == x_in) if modes[m] == "O" else (x != x_in))

    def stage_d(m, d):
        s = z if d == 0 else shards[d][0]
        copies = [partner_copy(m, d, s)]
        if d and modes[m] in "OC":
            copies += [
                remote(slot(m, s), slot(m, s), e_send.at[m, d, k], l_recv.at[m, s], tp_of(peer, core))
                for k, peer in enumerate(x_peers)
            ]

        def hand():
            if d == 0:
                pl.when(x != x_in)(lambda: arrived(slot(m, s), l_recv.at[m, s]))
            else:
                arrived(slot(m, s), l_recv.at[m, s])
            for copy in reversed(copies):
                copy.start()

        def drain():
            for copy in copies:
                copy.wait_send()

        pl.when(enters(m, d))(hand)
        finish.append(lambda: pl.when(enters(m, d))(drain))

    def stage_e(m, d):
        s = shards[d][0]
        here = (core == core_in) & jnp.logical_not(enters(m, d))
        copy = partner_copy(m, d, s)

        def hand():
            arrived(slot(m, s), l_recv.at[m, s])
            copy.start()

        pl.when(here)(hand)
        finish.append(lambda: pl.when(here)(copy.wait_send))

    def stage_end(m, d):
        s = z if d == 0 else shards[d][0]
        pl.when(core != core_in)(lambda: arrived(slot(m, s), l_recv.at[m, s]))

    def finalize(m, values):
        for i in range(prompts):
            mine(m, i)[...] = values[i]

            def keep(i=i):
                slot(m, z)[...] = values[i]

            pl.when(t * prompts + i == z)(keep)

    step_rows, pieces = 16, PIECES

    def norm(r, carry):
        at = pl.ds(pl.multiple_of(r * step_rows, step_rows), step_rows)
        wide = tok[at, :].astype(jnp.float32)
        scale = lax.rsqrt(jnp.mean(wide * wide, axis=-1, keepdims=True) + EPS)
        out = (wide * scale * in_gain[...]).astype(jnp.bfloat16)
        for b in range(n_sp):
            normed[b, at, :] = out[:, b * depth : (b + 1) * depth]
        return carry

    def norm_piece(k):
        need(fetch_gain)
        need(fetch_tok)
        turns = prompts * rows // step_rows // pieces
        lax.fori_loop(k * turns, (k + 1) * turns, norm, 0)

    def own_dot(g):
        first, width = spans[g]
        need(fetch_w)
        acc[g][...] = jnp.dot(
            normed[z], w_own[:, first : first + width], preferred_element_type=jnp.float32
        )

    def rope_item():
        need(fetch_rope)
        raw = jnp.zeros((ROPE, prompts * rows), jnp.float32)
        for b in range(n_sp):
            raw += lax.dot_general(
                w_rope[:, b * depth : (b + 1) * depth],
                normed[b],
                (((1,), (1,)), ((), ())),
                preferred_element_type=jnp.float32,
            )
        half = ROPE // 2
        index = lax.broadcasted_iota(jnp.int32, (half, rows), 1)
        channel = lax.broadcasted_iota(jnp.int32, (half, rows), 0)
        inverse = jnp.zeros((half, rows), jnp.float32)
        for c, value in enumerate(frequency):
            inverse = jnp.where(channel == c, value, inverse)
        values = []
        for i in range(prompts):
            position = offsets[i] + z * rows + index
            angle = position.astype(jnp.float32) * inverse
            sine, cosine = jnp.sin(angle), jnp.cos(angle)
            first = raw[:half, i * rows : (i + 1) * rows]
            second = raw[half:, i * rows : (i + 1) * rows]
            turned = [first * cosine - second * sine, second * cosine + first * sine]
            values.append(jnp.concatenate(turned, axis=0).astype(jnp.bfloat16))
        finalize(0, values)

    def group_item(g):
        value = acc[g][...].astype(jnp.bfloat16)
        finalize(g + 1, [value[i * rows : (i + 1) * rows] for i in range(prompts)])

    def latent_item(m):
        if m == 0:
            rope_item()
        else:
            group_item(m - 1)
        stage_l(m)

    stages = {
        "own": own_z,
        "norm": norm_piece,
        "odot": own_dot,
        "z": stage_z,
        "a": stage_a,
        "b": stage_b,
        "c": stage_c,
        "dot": stage_dot,
        "l": latent_item,
        "t": stage_t,
        "d": stage_d,
        "e": stage_e,
        "end": stage_end,
    }

    def run(schedule, middle):
        finish.clear()
        fetched.clear()
        for name, *args in schedule:
            if name == "a" and not middle:
                stage_z(*args)
            stages[name](*args)
            while len(finish) > PENDING:
                finish.pop(0)()
        for fn in finish:
            fn()

    if tuned:
        inner = has_up & has_down
        pl.when(inner)(lambda: run(MIDDLE, True))
        pl.when(jnp.logical_not(inner))(lambda: run(OUTER, False))
    else:
        run(plain_schedule(units, groups, n_sp), False)


def gather_latent(tokens, w_latent, w_rope, in_gain, offsets, frequency):
    prompts, rows, width = tokens.shape
    n_grp, n_sp, n_tp = (lax.axis_size(a) for a in ("grp", "sp", "tp"))
    n_x = n_tp // CORES
    depth, cols = w_latent.shape
    spans = column_groups(n_sp, cols)
    groups = len(spans)
    chunk = depth // (n_grp * n_tp)
    total = prompts * rows
    units = groups * (n_sp - 1)
    peers = max(n_x, n_grp) - 1
    others = max(n_x - 1, 1)
    items = groups + 1
    bf16, f32 = jnp.bfloat16, jnp.float32
    dma = pltpu.SemaphoreType.DMA
    stay = lambda a: pltpu.with_memory_space_constraint(a, pltpu.HBM)
    limit = (40 if groups > 1 else 60) * 1024 * 1024
    vmem = pl.BlockSpec(memory_space=pltpu.VMEM)
    hbm = pl.BlockSpec(memory_space=pltpu.HBM)
    return pl.pallas_call(
        functools.partial(gather_kernel, n_grp, n_sp, n_tp, spans, frequency),
        out_shape=(
            jax.ShapeDtypeStruct((n_sp, rows, cols), bf16),
            jax.ShapeDtypeStruct((n_sp, ROPE, rows), bf16),
        ),
        in_specs=[hbm, hbm, hbm, hbm, pl.BlockSpec(memory_space=pltpu.SMEM)],
        out_specs=(vmem, vmem),
        scratch_shapes=[
            pltpu.VMEM((total, width), bf16),
            pltpu.VMEM((depth, cols), bf16),
            pltpu.VMEM((ROPE, width), bf16),
            pltpu.VMEM((1, width), f32),
            pltpu.VMEM((n_sp, total, depth), bf16),
            *[pltpu.VMEM((n_sp, CORES, n_x, n_grp, chunk, w), bf16) for _, w in spans],
            *[pltpu.VMEM((total, w), f32) for _, w in spans],
            *[pltpu.VMEM((prompts, rows, w), bf16) for _, w in spans],
            *[pltpu.VMEM((others, prompts, rows, w), bf16) for _, w in spans],
            pltpu.VMEM((prompts, ROPE, rows), bf16),
            pltpu.VMEM((others, prompts, ROPE, rows), bf16),
            dma((4,)),
            dma((groups, 2)),
            dma((units,)),
            dma((groups, n_sp)),
            dma((units, peers)),
            dma((units, peers)),
            dma((units, peers)),
            dma((units, peers)),
            dma((units,)),
            dma((units,)),
            dma((items, prompts)),
            dma((items, others, prompts)),
            dma((items, others, prompts)),
            dma((items, prompts, others)),
            dma((items, n_sp, others)),
            dma((items, n_sp)),
            dma((items, n_sp)),
        ],
        compiler_params=pltpu.CompilerParams(
            collective_id=0, has_side_effects=True, vmem_limit_bytes=limit
        ),
    )(*map(stay, (tokens.reshape(total, width), w_latent, w_rope, in_gain)), offsets)


def cache_kernel(
    n_blocks,
    latent_ref,
    gain_ref,
    wk_ref,
    wv_ref,
    q_nope_ref,
    q_rope_ref,
    rope_ref,
    keys_ref,
    values_ref,
    rope_keys_ref,
    read_ref,
    scores,
    held,
):
    b = pl.program_id(0)
    heads = scores.shape[1]

    def per_head(row, size):
        wide = jnp.broadcast_to(row.astype(jnp.float32), (heads, heads * size))
        head = lax.broadcasted_iota(jnp.int32, wide.shape, 0)
        lane = lax.broadcasted_iota(jnp.int32, wide.shape, 1)
        return jnp.where((lane >= head * size) & (lane < head * size + size), wide, 0.0)

    query = per_head(q_nope_ref[...], HEAD).astype(jnp.bfloat16)
    spread = (heads * ROPE, ROPE)
    fold = lax.broadcasted_iota(jnp.int32, spread, 0) % ROPE == lax.broadcasted_iota(
        jnp.int32, spread, 1
    )
    rotary_q = jnp.dot(
        per_head(q_rope_ref[...], ROPE).astype(jnp.bfloat16),
        jnp.where(fold, 1.0, 0.0).astype(jnp.bfloat16),
        preferred_element_type=jnp.float32,
    ).astype(jnp.bfloat16)
    raw = latent_ref[0].astype(jnp.float32)
    scale = lax.rsqrt(jnp.mean(raw * raw, axis=-1, keepdims=True) + EPS)
    latent = (raw * scale * gain_ref[...]).astype(jnp.bfloat16)
    keys = jnp.dot(latent, wk_ref[...], preferred_element_type=jnp.float32).astype(jnp.bfloat16)
    keys_ref[...] = keys
    values = jnp.dot(latent, wv_ref[...], preferred_element_type=jnp.float32).astype(jnp.bfloat16)
    values_ref[...] = values
    held[b] = values
    rope = rope_ref[0]
    rope_keys_ref[...] = rope
    across = (((1,), (1,)), ((), ()))
    part = lax.dot_general(query, keys, across, preferred_element_type=jnp.float32)
    part += jnp.dot(rotary_q, rope, preferred_element_type=jnp.float32)
    scores[b] = part / jnp.sqrt(jnp.float32(HEAD + ROPE))

    @pl.when(b == n_blocks - 1)
    def _():
        every = scores[...]
        peak = jnp.max(jnp.max(every, axis=-1, keepdims=True), axis=0, keepdims=True)
        expo = jnp.exp(every - peak)
        total = jnp.sum(jnp.sum(expo, axis=-1, keepdims=True), axis=0, keepdims=True)
        weights = (expo / total).astype(jnp.bfloat16)
        out = jnp.dot(weights[0], held[0], preferred_element_type=jnp.float32)
        for i in range(1, n_blocks):
            out += jnp.dot(weights[i], held[i], preferred_element_type=jnp.float32)
        head = lax.broadcasted_iota(jnp.int32, out.shape, 0)
        lane = lax.broadcasted_iota(jnp.int32, out.shape, 1)
        picked = jnp.where((lane >= head * HEAD) & (lane < head * HEAD + HEAD), out, 0.0)
        read_ref[...] = jnp.sum(picked, axis=0, keepdims=True).astype(jnp.bfloat16)


def fill_cache(latent, kv_gain, w_up_key, w_up_value, q_nope, q_rope, rope):
    n_blocks, rows, cols = latent.shape
    out_cols = w_up_key.shape[1]
    heads = out_cols // HEAD
    length = n_blocks * rows
    whole = lambda shape: pl.BlockSpec(shape, lambda b: (0,) * len(shape))
    return pl.pallas_call(
        functools.partial(cache_kernel, n_blocks),
        grid=(n_blocks,),
        out_shape=(
            jax.ShapeDtypeStruct((length, out_cols), jnp.bfloat16),
            jax.ShapeDtypeStruct((length, out_cols), jnp.bfloat16),
            jax.ShapeDtypeStruct((ROPE, length), jnp.bfloat16),
            jax.ShapeDtypeStruct((1, out_cols), jnp.bfloat16),
        ),
        in_specs=[
            pl.BlockSpec((1, rows, cols), lambda b: (b, 0, 0)),
            whole((1, cols)),
            whole((cols, out_cols)),
            whole((cols, out_cols)),
            whole(q_nope.shape),
            whole(q_rope.shape),
            pl.BlockSpec((1, ROPE, rows), lambda b: (b, 0, 0)),
        ],
        out_specs=(
            pl.BlockSpec((rows, out_cols), lambda b: (b, 0)),
            pl.BlockSpec((rows, out_cols), lambda b: (b, 0)),
            pl.BlockSpec((ROPE, rows), lambda b: (0, b)),
            whole((1, out_cols)),
        ),
        scratch_shapes=[
            pltpu.VMEM((n_blocks, heads, rows), jnp.float32),
            pltpu.VMEM((n_blocks, rows, out_cols), jnp.bfloat16),
        ],
        compiler_params=pltpu.CompilerParams(vmem_limit_bytes=30 * 1024 * 1024),
    )(latent, kv_gain, w_up_key, w_up_value, q_nope, q_rope, rope)


def local(
    tokens, offsets, in_gain, w_latent, w_rope_key, kv_gain, w_up_key, w_up_value, q_nope, q_rope
):
    steps = -np.arange(0, ROPE, 2).astype(np.float32) / ROPE
    frequency = [float(f) for f in np.float32(10000.0) ** steps]
    latent, rope = gather_latent(tokens, w_latent, w_rope_key.T, in_gain[None], offsets, frequency)
    keys, values, rope_keys, read = fill_cache(
        latent, kv_gain[None], w_up_key, w_up_value, q_nope, q_rope, rope
    )
    return (keys[None], values[None], rope_keys[None], read)


def solution(mesh):
    in_specs = (
        P(("grp", "tp"), "sp", None),
        P(("grp", "tp")),
        P(),
        P("sp", None),
        P(),
        P(),
        P(None, "tp"),
        P(None, "tp"),
        P(("grp", "sp"), "tp"),
        P(("grp", "sp"), "tp"),
    )
    out_specs = (
        P(("grp", "sp"), None, "tp"),
        P(("grp", "sp"), None, "tp"),
        P(("grp", "sp"), None, None),
        P(("grp", "sp"), "tp"),
    )
    return jax.shard_map(local, mesh=mesh, in_specs=in_specs, out_specs=out_specs, check_vma=False)
```

```python
import functools

import jax
import jax.numpy as jnp
import numpy as np
from jax import lax
from jax.experimental import pallas as pl
from jax.experimental.pallas import tpu as pltpu
from jax.sharding import PartitionSpec as P

HEAD = 64
ROPE = 32
CORES = 2
PIECES = 4
PENDING = 60
PARTS = (1, 1, 1, 1, 1, 1, 1, 1)
MODES = ("F", "O", "F", "O", "C", "O", "C", "O", "O")
X_FIRST = (True, False, False, False, True, True, True, False, True, True, True, True, False, True, True, False, True, True, False, False, True, True, True, False)
OUTER = (
    ("own", 0), ("own", 4), ("own", 1), ("norm", 0), ("own", 2), ("norm", 3), ("own", 3),
    ("norm", 2), ("own", 5), ("a", 3), ("a", 0), ("a", 9), ("own", 6), ("a", 12), ("b", 3),
    ("b", 0), ("a", 6), ("a", 1), ("norm", 1), ("a", 4), ("odot", 2), ("own", 7), ("odot", 3),
    ("odot", 1), ("odot", 0), ("odot", 4), ("b", 9), ("odot", 5), ("b", 12), ("odot", 7), ("a", 10),
    ("c", 0), ("a", 15), ("b", 6), ("c", 3), ("b", 1), ("dot", 0), ("b", 4), ("a", 21), ("a", 13),
    ("dot", 3), ("c", 9), ("b", 10), ("a", 5), ("c", 12), ("a", 2), ("l", 0), ("b", 15), ("a", 8),
    ("c", 6), ("c", 1), ("b", 21), ("dot", 6), ("c", 4), ("b", 13), ("a", 7), ("a", 16), ("b", 5),
    ("b", 2), ("dot", 12), ("b", 8), ("dot", 4), ("t", 0), ("c", 10), ("odot", 6), ("a", 11),
    ("c", 15), ("c", 21), ("dot", 9), ("a", 19), ("dot", 1), ("a", 14), ("c", 13), ("b", 16),
    ("b", 7), ("dot", 21), ("a", 23), ("dot", 10), ("b", 11), ("c", 5), ("c", 2), ("a", 17),
    ("a", 22), ("dot", 15), ("c", 8), ("d", 0, 0), ("b", 14), ("dot", 5), ("l", 2), ("dot", 2),
    ("l", 1), ("dot", 8), ("c", 7), ("a", 20), ("b", 17), ("d", 0, 1), ("d", 0, 3), ("b", 22),
    ("d", 0, 2), ("dot", 7), ("l", 3), ("c", 11), ("b", 23), ("b", 19), ("dot", 11), ("l", 4),
    ("a", 18), ("t", 2), ("b", 20), ("c", 16), ("dot", 13), ("c", 22), ("dot", 16), ("c", 17),
    ("d", 3, 0), ("d", 1, 0), ("d", 1, 1), ("d", 1, 2), ("c", 19), ("dot", 22), ("dot", 17),
    ("l", 6), ("t", 4), ("c", 14), ("d", 3, 3), ("b", 18), ("c", 23), ("dot", 19), ("d", 3, 2),
    ("c", 20), ("d", 3, 1), ("dot", 14), ("l", 5), ("dot", 20), ("e", 3, 2), ("d", 2, 0),
    ("dot", 23), ("l", 8), ("d", 1, 3), ("e", 1, 2), ("d", 5, 2), ("d", 4, 0), ("t", 6),
    ("d", 4, 1), ("e", 3, 3), ("c", 18), ("d", 2, 2), ("d", 4, 3), ("dot", 18), ("l", 7),
    ("d", 2, 1), ("d", 8, 1), ("d", 5, 1), ("d", 5, 3), ("e", 1, 1), ("e", 3, 1), ("d", 8, 2),
    ("d", 8, 3), ("d", 8, 0), ("e", 1, 3), ("d", 4, 2), ("d", 5, 0), ("d", 7, 2), ("e", 5, 2),
    ("d", 6, 0), ("d", 7, 1), ("e", 4, 1), ("d", 6, 1), ("d", 2, 3), ("d", 6, 2), ("e", 4, 3),
    ("d", 7, 0), ("e", 5, 1), ("d", 7, 3), ("d", 6, 3), ("e", 6, 1), ("e", 5, 3), ("e", 8, 3),
    ("e", 8, 1), ("e", 7, 2), ("e", 4, 2), ("e", 6, 3), ("e", 7, 1), ("e", 8, 2), ("e", 6, 2),
    ("e", 7, 3), ("end", 0, 0), ("end", 0, 1), ("end", 0, 2), ("end", 0, 3), ("end", 1, 0),
    ("end", 1, 1), ("end", 1, 2), ("end", 1, 3), ("end", 2, 0), ("end", 2, 1), ("end", 2, 2),
    ("end", 2, 3), ("end", 3, 0), ("end", 3, 1), ("end", 3, 2), ("end", 3, 3), ("end", 4, 0),
    ("end", 4, 1), ("end", 4, 2), ("end", 4, 3), ("end", 5, 0), ("end", 5, 1), ("end", 5, 2),
    ("end", 5, 3), ("end", 6, 0), ("end", 6, 1), ("end", 6, 2), ("end", 6, 3), ("end", 7, 0),
    ("end", 7, 1), ("end", 7, 2), ("end", 7, 3), ("end", 8, 0), ("end", 8, 1), ("end", 8, 2),
    ("end", 8, 3),
)
MIDDLE = (
    ("own", 0), ("own", 1), ("norm", 0), ("norm", 1), ("own", 2), ("own", 3), ("norm", 3),
    ("own", 4), ("z", 0), ("a", 0), ("z", 1), ("a", 1), ("z", 4), ("a", 4), ("z", 3), ("a", 3),
    ("norm", 2), ("odot", 1), ("odot", 6), ("z", 6), ("a", 6), ("z", 7), ("z", 9), ("odot", 3),
    ("a", 7), ("a", 9), ("z", 10), ("a", 10), ("odot", 4), ("b", 1), ("own", 5), ("b", 4), ("b", 0),
    ("b", 3), ("odot", 5), ("z", 12), ("own", 7), ("z", 5), ("a", 5), ("b", 7), ("odot", 7),
    ("z", 13), ("a", 13), ("z", 2), ("a", 2), ("l", 0), ("a", 12), ("b", 10), ("odot", 0), ("b", 9),
    ("own", 6), ("z", 21), ("z", 8), ("a", 8), ("z", 16), ("a", 16), ("c", 4), ("c", 0), ("z", 15),
    ("a", 15), ("c", 3), ("dot", 4), ("z", 11), ("a", 11), ("z", 14), ("a", 14), ("odot", 2),
    ("b", 6), ("z", 19), ("a", 19), ("c", 10), ("dot", 10), ("z", 22), ("a", 22), ("dot", 0),
    ("c", 1), ("b", 2), ("b", 12), ("z", 17), ("a", 17), ("z", 18), ("a", 18), ("b", 5), ("b", 16),
    ("b", 8), ("b", 11), ("b", 13), ("c", 9), ("z", 23), ("a", 23), ("b", 22), ("t", 0), ("c", 7),
    ("b", 15), ("dot", 3), ("c", 2), ("dot", 2), ("c", 6), ("dot", 9), ("c", 5), ("b", 14),
    ("z", 20), ("a", 21), ("a", 20), ("b", 17), ("b", 18), ("dot", 1), ("l", 1), ("c", 16),
    ("dot", 16), ("dot", 7), ("b", 19), ("c", 12), ("dot", 5), ("l", 2), ("c", 8), ("b", 20),
    ("c", 11), ("c", 13), ("b", 23), ("c", 15), ("dot", 15), ("b", 21), ("c", 19), ("dot", 13),
    ("dot", 6), ("dot", 11), ("l", 4), ("dot", 8), ("l", 3), ("c", 23), ("d", 1, 2), ("t", 2),
    ("d", 2, 0), ("dot", 19), ("d", 2, 3), ("c", 14), ("c", 17), ("d", 3, 1), ("dot", 12),
    ("c", 21), ("d", 3, 3), ("dot", 23), ("dot", 14), ("l", 5), ("d", 1, 0), ("d", 1, 3), ("c", 22),
    ("d", 3, 2), ("e", 3, 1), ("t", 4), ("d", 4, 0), ("c", 18), ("d", 3, 0), ("d", 1, 1),
    ("d", 0, 3), ("dot", 17), ("l", 6), ("d", 5, 0), ("d", 5, 2), ("c", 20), ("dot", 21),
    ("dot", 22), ("l", 8), ("dot", 18), ("d", 4, 2), ("d", 2, 2), ("e", 1, 1), ("d", 4, 1),
    ("t", 6), ("d", 6, 0), ("d", 2, 1), ("e", 1, 3), ("d", 4, 3), ("d", 0, 1), ("dot", 20),
    ("l", 7), ("d", 5, 1), ("e", 1, 2), ("d", 5, 3), ("e", 5, 1), ("d", 8, 1), ("e", 4, 1),
    ("d", 6, 2), ("e", 3, 2), ("d", 6, 3), ("d", 0, 0), ("d", 8, 2), ("e", 4, 3), ("d", 7, 2),
    ("e", 5, 2), ("e", 3, 3), ("d", 6, 1), ("d", 8, 0), ("e", 5, 3), ("d", 0, 2), ("d", 7, 1),
    ("d", 7, 3), ("e", 7, 1), ("e", 7, 2), ("d", 8, 3), ("e", 6, 2), ("e", 4, 2), ("e", 8, 2),
    ("e", 7, 3), ("d", 7, 0), ("e", 6, 1), ("e", 8, 1), ("e", 6, 3), ("e", 8, 3), ("end", 0, 0),
    ("end", 0, 1), ("end", 0, 2), ("end", 0, 3), ("end", 1, 0), ("end", 1, 1), ("end", 1, 2),
    ("end", 1, 3), ("end", 2, 0), ("end", 2, 1), ("end", 2, 2), ("end", 2, 3), ("end", 3, 0),
    ("end", 3, 1), ("end", 3, 2), ("end", 3, 3), ("end", 4, 0), ("end", 4, 1), ("end", 4, 2),
    ("end", 4, 3), ("end", 5, 0), ("end", 5, 1), ("end", 5, 2), ("end", 5, 3), ("end", 6, 0),
    ("end", 6, 1), ("end", 6, 2), ("end", 6, 3), ("end", 7, 0), ("end", 7, 1), ("end", 7, 2),
    ("end", 7, 3), ("end", 8, 0), ("end", 8, 1), ("end", 8, 2), ("end", 8, 3),
)

EPS = 1e-06
MESH = pl.DeviceIdType.MESH


def column_groups(n_sp, cols):
    if n_sp > 4 or cols % 1024:
        return [(0, cols)]
    each, total, out = cols // sum(PARTS), 0, []
    for part in PARTS:
        out.append((total, part * each))
        total += part * each
    return out


def plain_schedule(units, groups, n_sp):
    late = len(units) * 10
    ops = [(g, ("own", g)) for g in range(groups)]
    ops += [(k, ("norm", k)) for k in range(PIECES)]
    ops += [(PIECES + g, ("odot", g)) for g in range(groups)]
    done = {}
    for u, (g, d) in enumerate(units):
        at = PIECES + 2 + u
        ops += [(at, ("a", u)), (at + 2, ("b", u)), (at + 4, ("c", u)), (at + 5, ("dot", u))]
        done[g + 1] = at + 5
    for m in range(groups + 1):
        at = done.get(m, PIECES + 1)
        ops += [(at + 0.5, ("l", m)), (at + 3, ("t", m))]
        ops += [(at + 6, ("d", m, d)) for d in range(n_sp)]
        ops += [(late + m, ("end", m, d)) for d in range(n_sp)]
    return [op for _, op in sorted(ops, key=lambda item: item[0])]


def gather_kernel(n_grp, n_sp, n_tp, spans, frequency, *refs):
    groups = len(spans)
    tok_hbm, w_hbm, w_rope_hbm, gain_hbm, offsets, lat_out, rope_out = refs[:7]
    tok, w_own, w_rope, in_gain, normed = refs[7:12]
    wbuf, acc, own, transit = (refs[12 + k * groups : 12 + (k + 1) * groups] for k in range(4))
    (
        own_rope,
        transit_rope,
        local_sem,
        own_send,
        z_send,
        z_recv,
        a_send,
        a_recv,
        b_send,
        b_recv,
        c_send,
        c_recv,
        l_send,
        t_send,
        t_recv,
        x_send,
        e_send,
        d_send,
        l_recv,
    ) = refs[12 + 4 * groups :]
    n_x = n_tp // CORES
    prompts, rows = own[0].shape[:2]
    depth, cols = w_own.shape
    chunk = depth // (n_grp * n_tp)
    y, z, t = lax.axis_index("grp"), lax.axis_index("sp"), lax.axis_index("tp")
    x, core = t // CORES, t % CORES
    rank = (core * n_x + x) * n_grp + y

    def tp_of(x_to, core_to):
        return {"tp": x_to * CORES + core_to}

    partner = tp_of(x, 1 - core)
    x_peers = [lax.rem(x + k, n_x) for k in range(1, n_x)]
    y_peers = [lax.rem(y + k, n_grp) for k in range(1, n_grp)]
    z_up, z_down = lax.rem(z + 1, n_sp), lax.rem(z + n_sp - 1, n_sp)
    has_up, has_down = z + 1 < n_sp, z > 0

    fetch_tok = pltpu.make_async_copy(tok_hbm, tok, local_sem.at[0])
    fetch_w = pltpu.make_async_copy(w_hbm, w_own, local_sem.at[1])
    fetch_rope = pltpu.make_async_copy(w_rope_hbm, w_rope, local_sem.at[2])
    fetch_gain = pltpu.make_async_copy(gain_hbm, in_gain, local_sem.at[3])

    barrier = pltpu.get_barrier_semaphore()

    def greet(target):
        pl.semaphore_signal(barrier, inc=1, device_id=target, device_id_type=MESH)

    pl.when(has_up)(lambda: greet({"sp": z_up}))
    pl.when(has_down)(lambda: greet({"sp": z_down}))
    near = [tp_of(p, core) for p in x_peers] + [{"grp": p} for p in y_peers] + [partner]
    for target in near:
        greet(target)
    fetch_gain.start()
    fetch_tok.start()
    fetch_w.start()
    fetch_rope.start()
    pl.semaphore_wait(barrier, len(near) + has_up.astype(jnp.int32) + has_down.astype(jnp.int32))

    finish, fetched = [], []
    tuned = n_sp == 4 and groups == len(PARTS)
    modes = MODES if tuned else ("F",) * (groups + 1)

    def remote(src, dst, send, recv, device):
        return pltpu.make_async_remote_copy(
            src_ref=src,
            dst_ref=dst,
            send_sem=send,
            recv_sem=recv,
            device_id=device,
            device_id_type=MESH,
        )

    def arrived(ref, recv):
        remote(ref, ref, recv, recv, partner).wait_recv()

    def need(copy):
        if not any(copy is other for other in fetched):
            fetched.append(copy)
            copy.wait()

    def begin(copy, when=None):
        if when is None:
            copy.start()
            finish.append(copy.wait_send)
        else:
            pl.when(when)(copy.start)
            finish.append(lambda: pl.when(when)(copy.wait_send))

    units = [(g, d) for g in range(groups) for d in range(1, n_sp)]
    above = n_sp - 1 - z
    both = jnp.minimum(z, above)

    def shard(d):
        paired = d <= 2 * both
        hop = jnp.where(paired, (d + 1) // 2, d - both)
        up = jnp.where(paired, d % 2 == 1, above > z)
        return jnp.where(up, z + hop, z - hop), up

    shards = {d: shard(d) for d in range(1, n_sp)}

    def own_z(g):
        first, width = spans[g]
        for side, ahead, exists in ((0, z_up, has_up), (1, z_down, has_down)):
            copy = remote(
                w_hbm.at[pl.ds(rank * chunk, chunk), pl.ds(first, width)],
                wbuf[g].at[z, core, x, y],
                own_send.at[g, side],
                z_recv.at[g, z],
                {"sp": ahead},
            )
            begin(copy, exists)

    def x_first(u):
        return X_FIRST[u] if tuned else u % 4 > 0

    def spread(u, src, send, recv, along_x):
        peers = x_peers if along_x else y_peers
        for k, peer in enumerate(peers):
            device = tp_of(peer, core) if along_x else {"grp": peer}
            begin(remote(src, src, send.at[u, k], recv.at[u, k], device))

    def block_a(u):
        g, d = units[u]
        return wbuf[g].at[shards[d][0], core, x, y]

    def block_b(u):
        g, d = units[u]
        if x_first(u):
            return wbuf[g].at[shards[d][0], core, :, y]
        return wbuf[g].at[shards[d][0], core, x]

    def stage_z(u):
        g, d = units[u]
        s, up = shards[d]
        arrived(block_a(u), z_recv.at[g, s])
        exists = jnp.where(up, has_down, has_up)
        ahead = jnp.where(up, z_down, z_up)
        begin(
            remote(block_a(u), block_a(u), z_send.at[u], z_recv.at[g, s], {"sp": ahead}), exists
        )

    def stage_a(u):
        spread(u, block_a(u), a_send, a_recv, x_first(u))

    def stage_b(u):
        for k in range(len(x_peers if x_first(u) else y_peers)):
            arrived(block_a(u), a_recv.at[u, k])
        spread(u, block_b(u), b_send, b_recv, not x_first(u))

    def stage_c(u):
        g, d = units[u]
        for k in range(len(y_peers if x_first(u) else x_peers)):
            arrived(block_b(u), b_recv.at[u, k])
        ref = wbuf[g].at[shards[d][0], core]
        begin(remote(ref, ref, c_send.at[u], c_recv.at[u], partner))

    def stage_dot(u):
        g, d = units[u]
        s, _ = shards[d]
        arrived(wbuf[g].at[s, core], c_recv.at[u])
        weight = wbuf[g][s].reshape(depth, spans[g][1])
        acc[g][...] += jnp.dot(normed[s], weight, preferred_element_type=jnp.float32)

    def slot(m, s):
        if m == 0:
            return rope_out.at[s]
        first, width = spans[m - 1]
        return lat_out.at[s, :, pl.ds(first, width)]

    def mine(m, i):
        return own_rope.at[i] if m == 0 else own[m - 1].at[i]

    def held(m, k, i):
        return transit_rope.at[k, i] if m == 0 else transit[m - 1].at[k, i]

    def stage_l(m):
        for i in range(prompts):
            home = t * prompts + i
            if modes[m] != "C":
                copy = remote(
                    mine(m, i), slot(m, z), l_send.at[m, i], l_recv.at[m, z], {"sp": home}
                )
                begin(copy, home != z)
            for k, peer in enumerate(x_peers):
                device = tp_of(peer, core)
                beside = remote(mine(m, i), slot(m, z), x_send.at[m, i, k], l_recv.at[m, z], device)
                begin(beside, home == z)
                if modes[m] == "D":
                    routed = remote(
                        mine(m, i),
                        slot(m, z),
                        x_send.at[m, i, k],
                        l_recv.at[m, z],
                        device | {"sp": home},
                    )
                    begin(routed, home != z)
                elif modes[m] != "O":
                    across = remote(
                        mine(m, i), held(m, k, i), x_send.at[m, i, k], t_recv.at[m, k, i], device
                    )
                    begin(across, home != z)

    def stage_t(m):
        if modes[m] not in "FC":
            return
        for k in range(n_x - 1):
            source = lax.rem(x + n_x - 1 - k, n_x) * CORES + core
            for i in range(prompts):
                home = source * prompts + i
                copy = remote(
                    held(m, k, i), slot(m, z), t_send.at[m, k, i], l_recv.at[m, z], {"sp": home}
                )

                def pass_on(k=k, i=i, copy=copy):
                    arrived(held(m, k, i), t_recv.at[m, k, i])
                    copy.start()

                pl.when(home != z)(pass_on)
                finish.append(lambda home=home, copy=copy: pl.when(home != z)(copy.wait_send))

    owner = z // prompts
    x_in, core_in = owner // CORES, owner % CORES

    def partner_copy(m, d, s):
        return remote(slot(m, s), slot(m, s), d_send.at[m, d], l_recv.at[m, s], partner)

    def enters(m, d):
        here = core == core_in
        if d == 0 or modes[m] in "FD":
            return here
        return here & ((x == x_in) if modes[m] == "O" else (x != x_in))

    def stage_d(m, d):
        s = z if d == 0 else shards[d][0]
        copies = [partner_copy(m, d, s)]
        if d and modes[m] in "OC":
            copies += [
                remote(slot(m, s), slot(m, s), e_send.at[m, d, k], l_recv.at[m, s], tp_of(peer, core))
                for k, peer in enumerate(x_peers)
            ]

        def hand():
            if d == 0:
                pl.when(x != x_in)(lambda: arrived(slot(m, s), l_recv.at[m, s]))
            else:
                arrived(slot(m, s), l_recv.at[m, s])
            for copy in reversed(copies):
                copy.start()

        def drain():
            for copy in copies:
                copy.wait_send()

        pl.when(enters(m, d))(hand)
        finish.append(lambda: pl.when(enters(m, d))(drain))

    def stage_e(m, d):
        s = shards[d][0]
        here = (core == core_in) & jnp.logical_not(enters(m, d))
        copy = partner_copy(m, d, s)

        def hand():
            arrived(slot(m, s), l_recv.at[m, s])
            copy.start()

        pl.when(here)(hand)
        finish.append(lambda: pl.when(here)(copy.wait_send))

    def stage_end(m, d):
        s = z if d == 0 else shards[d][0]
        pl.when(core != core_in)(lambda: arrived(slot(m, s), l_recv.at[m, s]))

    def finalize(m, values):
        for i in range(prompts):
            mine(m, i)[...] = values[i]

            def keep(i=i):
                slot(m, z)[...] = values[i]

            pl.when(t * prompts + i == z)(keep)

    step_rows, pieces = 16, PIECES

    def norm(r, carry):
        at = pl.ds(pl.multiple_of(r * step_rows, step_rows), step_rows)
        wide = tok[at, :].astype(jnp.float32)
        scale = lax.rsqrt(jnp.mean(wide * wide, axis=-1, keepdims=True) + EPS)
        out = (wide * scale * in_gain[...]).astype(jnp.bfloat16)
        for b in range(n_sp):
            normed[b, at, :] = out[:, b * depth : (b + 1) * depth]
        return carry

    def norm_piece(k):
        need(fetch_gain)
        need(fetch_tok)
        turns = prompts * rows // step_rows // pieces
        lax.fori_loop(k * turns, (k + 1) * turns, norm, 0)

    def own_dot(g):
        first, width = spans[g]
        need(fetch_w)
        acc[g][...] = jnp.dot(
            normed[z], w_own[:, first : first + width], preferred_element_type=jnp.float32
        )

    def rope_item():
        need(fetch_rope)
        raw = jnp.zeros((ROPE, prompts * rows), jnp.float32)
        for b in range(n_sp):
            raw += lax.dot_general(
                w_rope[:, b * depth : (b + 1) * depth],
                normed[b],
                (((1,), (1,)), ((), ())),
                preferred_element_type=jnp.float32,
            )
        half = ROPE // 2
        index = lax.broadcasted_iota(jnp.int32, (half, rows), 1)
        channel = lax.broadcasted_iota(jnp.int32, (half, rows), 0)
        inverse = jnp.zeros((half, rows), jnp.float32)
        for c, value in enumerate(frequency):
            inverse = jnp.where(channel == c, value, inverse)
        values = []
        for i in range(prompts):
            position = offsets[i] + z * rows + index
            angle = position.astype(jnp.float32) * inverse
            sine, cosine = jnp.sin(angle), jnp.cos(angle)
            first = raw[:half, i * rows : (i + 1) * rows]
            second = raw[half:, i * rows : (i + 1) * rows]
            turned = [first * cosine - second * sine, second * cosine + first * sine]
            values.append(jnp.concatenate(turned, axis=0).astype(jnp.bfloat16))
        finalize(0, values)

    def group_item(g):
        value = acc[g][...].astype(jnp.bfloat16)
        finalize(g + 1, [value[i * rows : (i + 1) * rows] for i in range(prompts)])

    def latent_item(m):
        if m == 0:
            rope_item()
        else:
            group_item(m - 1)
        stage_l(m)

    stages = {
        "own": own_z,
        "norm": norm_piece,
        "odot": own_dot,
        "z": stage_z,
        "a": stage_a,
        "b": stage_b,
        "c": stage_c,
        "dot": stage_dot,
        "l": latent_item,
        "t": stage_t,
        "d": stage_d,
        "e": stage_e,
        "end": stage_end,
    }

    def run(schedule, middle):
        finish.clear()
        fetched.clear()
        for name, *args in schedule:
            if name == "a" and not middle:
                stage_z(*args)
            stages[name](*args)
            while len(finish) > PENDING:
                finish.pop(0)()
        for fn in finish:
            fn()

    if tuned:
        inner = has_up & has_down
        pl.when(inner)(lambda: run(MIDDLE, True))
        pl.when(jnp.logical_not(inner))(lambda: run(OUTER, False))
    else:
        run(plain_schedule(units, groups, n_sp), False)


def gather_latent(tokens, w_latent, w_rope, in_gain, offsets, frequency):
    prompts, rows, width = tokens.shape
    n_grp, n_sp, n_tp = (lax.axis_size(a) for a in ("grp", "sp", "tp"))
    n_x = n_tp // CORES
    depth, cols = w_latent.shape
    spans = column_groups(n_sp, cols)
    groups = len(spans)
    chunk = depth // (n_grp * n_tp)
    total = prompts * rows
    units = groups * (n_sp - 1)
    peers = max(n_x, n_grp) - 1
    others = max(n_x - 1, 1)
    items = groups + 1
    bf16, f32 = jnp.bfloat16, jnp.float32
    dma = pltpu.SemaphoreType.DMA
    stay = lambda a: pltpu.with_memory_space_constraint(a, pltpu.HBM)
    limit = (40 if groups > 1 else 60) * 1024 * 1024
    vmem = pl.BlockSpec(memory_space=pltpu.VMEM)
    hbm = pl.BlockSpec(memory_space=pltpu.HBM)
    return pl.pallas_call(
        functools.partial(gather_kernel, n_grp, n_sp, n_tp, spans, frequency),
        out_shape=(
            jax.ShapeDtypeStruct((n_sp, rows, cols), bf16),
            jax.ShapeDtypeStruct((n_sp, ROPE, rows), bf16),
        ),
        in_specs=[hbm, hbm, hbm, hbm, pl.BlockSpec(memory_space=pltpu.SMEM)],
        out_specs=(vmem, vmem),
        scratch_shapes=[
            pltpu.VMEM((total, width), bf16),
            pltpu.VMEM((depth, cols), bf16),
            pltpu.VMEM((ROPE, width), bf16),
            pltpu.VMEM((1, width), f32),
            pltpu.VMEM((n_sp, total, depth), bf16),
            *[pltpu.VMEM((n_sp, CORES, n_x, n_grp, chunk, w), bf16) for _, w in spans],
            *[pltpu.VMEM((total, w), f32) for _, w in spans],
            *[pltpu.VMEM((prompts, rows, w), bf16) for _, w in spans],
            *[pltpu.VMEM((others, prompts, rows, w), bf16) for _, w in spans],
            pltpu.VMEM((prompts, ROPE, rows), bf16),
            pltpu.VMEM((others, prompts, ROPE, rows), bf16),
            dma((4,)),
            dma((groups, 2)),
            dma((units,)),
            dma((groups, n_sp)),
            dma((units, peers)),
            dma((units, peers)),
            dma((units, peers)),
            dma((units, peers)),
            dma((units,)),
            dma((units,)),
            dma((items, prompts)),
            dma((items, others, prompts)),
            dma((items, others, prompts)),
            dma((items, prompts, others)),
            dma((items, n_sp, others)),
            dma((items, n_sp)),
            dma((items, n_sp)),
        ],
        compiler_params=pltpu.CompilerParams(
            collective_id=0, has_side_effects=True, vmem_limit_bytes=limit
        ),
    )(*map(stay, (tokens.reshape(total, width), w_latent, w_rope, in_gain)), offsets)


def cache_kernel(
    latent_ref,
    gain_ref,
    wk_ref,
    wv_ref,
    q_nope_ref,
    q_rope_ref,
    rope_ref,
    keys_hbm,
    values_hbm,
    rope_keys_ref,
    read_ref,
    latents,
    keys,
    values,
    sems,
):
    n_blocks, rows, out_cols = keys.shape
    heads = out_cols // HEAD

    def per_head(row, size):
        wide = jnp.broadcast_to(row.astype(jnp.float32), (heads, heads * size))
        head = lax.broadcasted_iota(jnp.int32, wide.shape, 0)
        lane = lax.broadcasted_iota(jnp.int32, wide.shape, 1)
        return jnp.where((lane >= head * size) & (lane < head * size + size), wide, 0.0)

    def put(b, source, target, kind):
        copy = pltpu.make_async_copy(
            source.at[b], target.at[pl.ds(b * rows, rows), :], sems.at[kind, b]
        )
        copy.start()
        return copy

    query = per_head(q_nope_ref[...], HEAD).astype(jnp.bfloat16)
    spread = (heads * ROPE, ROPE)
    fold = lax.broadcasted_iota(jnp.int32, spread, 0) % ROPE == lax.broadcasted_iota(
        jnp.int32, spread, 1
    )
    rotary_q = jnp.dot(
        per_head(q_rope_ref[...], ROPE).astype(jnp.bfloat16),
        jnp.where(fold, 1.0, 0.0).astype(jnp.bfloat16),
        preferred_element_type=jnp.float32,
    ).astype(jnp.bfloat16)
    across = (((1,), (1,)), ((), ()))
    copies, scores = [], []

    def normalize(b):
        raw = latent_ref[b].astype(jnp.float32)
        scale = lax.rsqrt(jnp.mean(raw * raw, axis=-1, keepdims=True) + EPS)
        latents[b] = (raw * scale * gain_ref[...]).astype(jnp.bfloat16)

    def up_key(b):
        block = jnp.dot(latents[b], wk_ref[...], preferred_element_type=jnp.float32)
        keys[b] = block.astype(jnp.bfloat16)
        copies.append(put(b, keys, keys_hbm, 0))

    def up_value(b):
        block = jnp.dot(latents[b], wv_ref[...], preferred_element_type=jnp.float32)
        values[b] = block.astype(jnp.bfloat16)
        copies.append(put(b, values, values_hbm, 1))

    def score(b):
        part = lax.dot_general(query, keys[b], across, preferred_element_type=jnp.float32)
        part += jnp.dot(rotary_q, rope_ref[b], preferred_element_type=jnp.float32)
        scores.append(part / jnp.sqrt(jnp.float32(HEAD + ROPE)))
        rope_keys_ref[:, b * rows : (b + 1) * rows] = rope_ref[b]

    normalize(0)
    for b in range(n_blocks):
        if b + 1 < n_blocks:
            normalize(b + 1)
        up_key(b)
        if b + 1 < n_blocks:
            up_value(b)
        score(b)
    up_value(n_blocks - 1)
    peak = functools.reduce(jnp.maximum, scores).max(axis=-1, keepdims=True)
    expos = [jnp.exp(part - peak) for part in scores]
    total = functools.reduce(jnp.add, expos).sum(axis=-1, keepdims=True)
    out = jnp.zeros((heads, out_cols), jnp.float32)
    for b in range(n_blocks):
        weights = (expos[b] / total).astype(jnp.bfloat16)
        out += jnp.dot(weights, values[b], preferred_element_type=jnp.float32)
    head = lax.broadcasted_iota(jnp.int32, out.shape, 0)
    lane = lax.broadcasted_iota(jnp.int32, out.shape, 1)
    picked = jnp.where((lane >= head * HEAD) & (lane < head * HEAD + HEAD), out, 0.0)
    read_ref[...] = jnp.sum(picked, axis=0, keepdims=True).astype(jnp.bfloat16)
    for copy in copies:
        copy.wait()


def fill_cache(latent, kv_gain, w_up_key, w_up_value, q_nope, q_rope, rope):
    n_blocks, rows, cols = latent.shape
    out_cols = w_up_key.shape[1]
    length = n_blocks * rows
    vmem = pl.BlockSpec(memory_space=pltpu.VMEM)
    hbm = pl.BlockSpec(memory_space=pltpu.HBM)
    return pl.pallas_call(
        cache_kernel,
        out_shape=(
            jax.ShapeDtypeStruct((length, out_cols), jnp.bfloat16),
            jax.ShapeDtypeStruct((length, out_cols), jnp.bfloat16),
            jax.ShapeDtypeStruct((ROPE, length), jnp.bfloat16),
            jax.ShapeDtypeStruct((1, out_cols), jnp.bfloat16),
        ),
        in_specs=[vmem] * 7,
        out_specs=(hbm, hbm, vmem, vmem),
        scratch_shapes=[
            pltpu.VMEM((n_blocks, rows, cols), jnp.bfloat16),
            pltpu.VMEM((n_blocks, rows, out_cols), jnp.bfloat16),
            pltpu.VMEM((n_blocks, rows, out_cols), jnp.bfloat16),
            pltpu.SemaphoreType.DMA((2, n_blocks)),
        ],
        compiler_params=pltpu.CompilerParams(vmem_limit_bytes=40 * 1024 * 1024),
    )(latent, kv_gain, w_up_key, w_up_value, q_nope, q_rope, rope)


def local(
    tokens, offsets, in_gain, w_latent, w_rope_key, kv_gain, w_up_key, w_up_value, q_nope, q_rope
):
    steps = -np.arange(0, ROPE, 2).astype(np.float32) / ROPE
    frequency = [float(f) for f in np.float32(10000.0) ** steps]
    latent, rope = gather_latent(tokens, w_latent, w_rope_key.T, in_gain[None], offsets, frequency)
    keys, values, rope_keys, read = fill_cache(
        latent, kv_gain[None], w_up_key, w_up_value, q_nope, q_rope, rope
    )
    return (keys[None], values[None], rope_keys[None], read)


def solution(mesh):
    in_specs = (
        P(("grp", "tp"), "sp", None),
        P(("grp", "tp")),
        P(),
        P("sp", None),
        P(),
        P(),
        P(None, "tp"),
        P(None, "tp"),
        P(("grp", "sp"), "tp"),
        P(("grp", "sp"), "tp"),
    )
    out_specs = (
        P(("grp", "sp"), None, "tp"),
        P(("grp", "sp"), None, "tp"),
        P(("grp", "sp"), None, None),
        P(("grp", "sp"), "tp"),
    )
    return jax.shard_map(local, mesh=mesh, in_specs=in_specs, out_specs=out_specs, check_vma=False)
```

```python
import functools

import jax
import jax.numpy as jnp
import numpy as np
from jax import lax
from jax.experimental import pallas as pl
from jax.experimental.pallas import tpu as pltpu
from jax.sharding import PartitionSpec as P

HEAD = 64
ROPE = 32
CORES = 2
PIECES = 4
PENDING = 60
PARTS = (1, 1, 1, 1, 1, 1, 1, 1)
MODES = ("M", "F", "M", "M", "F", "M", "F", "O", "F")
DOUBLED = (False, False, False, False, True, False, True, True)
X_FIRST = (False, True, True, True, True, True, True, False, True, False, True, True, False, False, True, False, True, True, False, False, True, False, True, True)
OUTER = (
    ("own", 2), ("norm", 1), ("own", 0), ("own", 1), ("norm", 2), ("norm", 0), ("norm", 3),
    ("odot", 0), ("odot", 5), ("a", 3), ("a", 6), ("a", 0), ("odot", 6), ("odot", 1), ("odot", 2),
    ("odot", 7), ("odot", 3), ("own", 3), ("own", 4), ("b", 3), ("b", 6), ("b", 0), ("a", 7),
    ("own", 5), ("a", 1), ("a", 9), ("a", 4), ("c", 0), ("a", 2), ("odot", 4), ("own", 6), ("l", 0),
    ("a", 12), ("b", 1), ("b", 9), ("b", 4), ("own", 7), ("a", 5), ("c", 3), ("a", 10), ("a", 8),
    ("a", 15), ("c", 6), ("dot", 0), ("dot", 3), ("b", 7), ("c", 9), ("b", 2), ("t", 0), ("a", 13),
    ("b", 13), ("c", 1), ("a", 11), ("b", 12), ("c", 12), ("c", 4), ("d", 0, 2), ("dot", 6),
    ("dot", 9), ("a", 18), ("b", 10), ("d", 0, 0), ("b", 15), ("b", 5), ("dot", 1), ("d", 0, 1),
    ("b", 18), ("dot", 12), ("b", 8), ("dot", 4), ("c", 7), ("a", 14), ("c", 2), ("a", 16),
    ("dot", 7), ("d", 0, 3), ("b", 11), ("e", 0, 2), ("c", 13), ("dot", 13), ("a", 21), ("a", 19),
    ("c", 10), ("a", 17), ("c", 15), ("dot", 2), ("l", 1), ("b", 16), ("e", 0, 3), ("e", 0, 1),
    ("c", 5), ("b", 21), ("c", 8), ("a", 22), ("dot", 10), ("dot", 5), ("l", 2), ("c", 11),
    ("dot", 8), ("l", 3), ("dot", 15), ("a", 20), ("c", 18), ("t", 1), ("b", 17), ("c", 21),
    ("dot", 18), ("b", 14), ("c", 14), ("dot", 11), ("l", 4), ("b", 20), ("t", 3), ("a", 23),
    ("dot", 14), ("l", 5), ("b", 19), ("c", 19), ("c", 20), ("d", 3, 0), ("dot", 21), ("t", 2),
    ("c", 16), ("dot", 16), ("c", 17), ("d", 2, 2), ("d", 2, 0), ("dot", 20), ("b", 23), ("c", 23),
    ("d", 1, 1), ("t", 5), ("t", 4), ("dot", 19), ("l", 7), ("d", 1, 0), ("d", 4, 0), ("d", 3, 3),
    ("dot", 17), ("l", 6), ("dot", 23), ("d", 5, 0), ("d", 2, 3), ("d", 1, 2), ("b", 22), ("c", 22),
    ("d", 5, 3), ("d", 2, 1), ("e", 2, 2), ("dot", 22), ("l", 8), ("d", 3, 1), ("d", 5, 1),
    ("d", 5, 2), ("d", 4, 1), ("d", 3, 2), ("e", 3, 1), ("e", 3, 3), ("d", 1, 3), ("d", 7, 3),
    ("e", 2, 1), ("d", 4, 3), ("d", 4, 2), ("d", 7, 0), ("d", 7, 2), ("t", 6), ("d", 6, 1),
    ("d", 6, 2), ("d", 7, 1), ("d", 6, 3), ("d", 6, 0), ("e", 7, 3), ("e", 5, 1), ("e", 2, 3),
    ("t", 8), ("e", 7, 1), ("e", 5, 3), ("e", 3, 2), ("e", 5, 2), ("d", 8, 1), ("e", 7, 2),
    ("d", 8, 0), ("d", 8, 2), ("d", 8, 3), ("end", 0, 0), ("end", 0, 1), ("end", 0, 2),
    ("end", 0, 3), ("end", 1, 0), ("end", 1, 1), ("end", 1, 2), ("end", 1, 3), ("end", 2, 0),
    ("end", 2, 1), ("end", 2, 2), ("end", 2, 3), ("end", 3, 0), ("end", 3, 1), ("end", 3, 2),
    ("end", 3, 3), ("end", 4, 0), ("end", 4, 1), ("end", 4, 2), ("end", 4, 3), ("end", 5, 0),
    ("end", 5, 1), ("end", 5, 2), ("end", 5, 3), ("end", 6, 0), ("end", 6, 1), ("end", 6, 2),
    ("end", 6, 3), ("end", 7, 0), ("end", 7, 1), ("end", 7, 2), ("end", 7, 3), ("end", 8, 0),
    ("end", 8, 1), ("end", 8, 2), ("end", 8, 3),
)
MIDDLE = (
    ("own", 0), ("norm", 0), ("own", 1), ("norm", 1), ("own", 2), ("norm", 2), ("norm", 3),
    ("z", 6), ("z", 1), ("z", 0), ("own", 3), ("z", 4), ("z", 3), ("z", 7), ("a", 1), ("odot", 5),
    ("odot", 0), ("a", 3), ("odot", 1), ("odot", 2), ("a", 0), ("odot", 4), ("odot", 7), ("own", 4),
    ("a", 6), ("odot", 3), ("odot", 6), ("z", 2), ("b", 1), ("b", 0), ("z", 9), ("b", 3), ("z", 5),
    ("a", 7), ("a", 2), ("l", 0), ("own", 5), ("z", 10), ("z", 8), ("a", 4), ("a", 9), ("c", 1),
    ("c", 0), ("a", 5), ("z", 13), ("z", 12), ("a", 10), ("a", 12), ("b", 12), ("a", 8), ("a", 13),
    ("b", 13), ("b", 6), ("z", 11), ("own", 6), ("c", 3), ("t", 0), ("d", 0, 0), ("b", 7),
    ("z", 15), ("b", 2), ("a", 11), ("dot", 3), ("b", 4), ("z", 16), ("own", 7), ("dot", 1),
    ("dot", 0), ("b", 9), ("c", 6), ("b", 5), ("d", 0, 3), ("z", 14), ("a", 16), ("c", 7), ("c", 4),
    ("c", 2), ("b", 10), ("z", 21), ("a", 15), ("z", 19), ("b", 8), ("c", 12), ("c", 13), ("z", 17),
    ("a", 14), ("b", 14), ("b", 11), ("dot", 4), ("z", 22), ("a", 17), ("c", 9), ("d", 0, 2),
    ("z", 18), ("a", 19), ("b", 19), ("a", 18), ("dot", 7), ("dot", 2), ("l", 1), ("c", 10),
    ("d", 0, 1), ("z", 20), ("b", 15), ("dot", 13), ("c", 5), ("dot", 9), ("b", 16), ("b", 18),
    ("dot", 12), ("e", 0, 3), ("dot", 5), ("l", 2), ("dot", 6), ("c", 8), ("a", 22), ("a", 20),
    ("b", 20), ("t", 1), ("e", 0, 2), ("c", 14), ("c", 11), ("a", 21), ("z", 23), ("a", 23),
    ("c", 19), ("b", 21), ("b", 17), ("dot", 10), ("c", 18), ("dot", 8), ("l", 3), ("dot", 14),
    ("l", 5), ("c", 16), ("b", 22), ("e", 0, 1), ("c", 15), ("dot", 11), ("l", 4), ("dot", 19),
    ("b", 23), ("c", 21), ("c", 22), ("c", 23), ("t", 3), ("dot", 15), ("c", 20), ("dot", 16),
    ("c", 17), ("dot", 21), ("d", 3, 3), ("d", 3, 0), ("t", 2), ("d", 2, 0), ("d", 2, 1),
    ("d", 2, 3), ("dot", 20), ("dot", 18), ("l", 7), ("d", 3, 2), ("dot", 17), ("l", 6),
    ("d", 3, 1), ("t", 4), ("d", 4, 0), ("d", 1, 2), ("d", 1, 0), ("d", 2, 2), ("e", 2, 3),
    ("dot", 22), ("t", 5), ("d", 5, 0), ("d", 1, 1), ("d", 7, 0), ("d", 1, 3), ("d", 5, 2),
    ("dot", 23), ("l", 8), ("d", 5, 1), ("d", 4, 2), ("d", 4, 1), ("e", 3, 1), ("d", 7, 1),
    ("e", 2, 2), ("e", 3, 2), ("e", 2, 1), ("d", 5, 3), ("t", 6), ("d", 6, 1), ("d", 7, 3),
    ("t", 8), ("d", 7, 2), ("e", 7, 1), ("e", 7, 3), ("d", 6, 2), ("e", 5, 3), ("e", 3, 3),
    ("d", 4, 3), ("e", 5, 2), ("e", 5, 1), ("d", 6, 3), ("d", 6, 0), ("e", 7, 2), ("d", 8, 2),
    ("d", 8, 1), ("d", 8, 3), ("d", 8, 0), ("end", 0, 0), ("end", 0, 1), ("end", 0, 2),
    ("end", 0, 3), ("end", 1, 0), ("end", 1, 1), ("end", 1, 2), ("end", 1, 3), ("end", 2, 0),
    ("end", 2, 1), ("end", 2, 2), ("end", 2, 3), ("end", 3, 0), ("end", 3, 1), ("end", 3, 2),
    ("end", 3, 3), ("end", 4, 0), ("end", 4, 1), ("end", 4, 2), ("end", 4, 3), ("end", 5, 0),
    ("end", 5, 1), ("end", 5, 2), ("end", 5, 3), ("end", 6, 0), ("end", 6, 1), ("end", 6, 2),
    ("end", 6, 3), ("end", 7, 0), ("end", 7, 1), ("end", 7, 2), ("end", 7, 3), ("end", 8, 0),
    ("end", 8, 1), ("end", 8, 2), ("end", 8, 3),
)

EPS = 1e-06
MESH = pl.DeviceIdType.MESH


def column_groups(n_sp, cols):
    if n_sp > 4 or cols % 1024:
        return [(0, cols)]
    each, total, out = cols // sum(PARTS), 0, []
    for part in PARTS:
        out.append((total, part * each))
        total += part * each
    return out


def plain_schedule(units, groups, n_sp):
    late = len(units) * 10
    ops = [(g, ("own", g)) for g in range(groups)]
    ops += [(k, ("norm", k)) for k in range(PIECES)]
    ops += [(PIECES + g, ("odot", g)) for g in range(groups)]
    done = {}
    for u, (g, d) in enumerate(units):
        at = PIECES + 2 + u
        ops += [(at, ("a", u)), (at + 2, ("b", u)), (at + 4, ("c", u)), (at + 5, ("dot", u))]
        done[g + 1] = at + 5
    for m in range(groups + 1):
        at = done.get(m, PIECES + 1)
        ops += [(at + 0.5, ("l", m)), (at + 3, ("t", m))]
        ops += [(at + 6, ("d", m, d)) for d in range(n_sp)]
        ops += [(late + m, ("end", m, d)) for d in range(n_sp)]
    return [op for _, op in sorted(ops, key=lambda item: item[0])]


def gather_kernel(n_grp, n_sp, n_tp, spans, frequency, *refs):
    groups = len(spans)
    tok_hbm, w_hbm, w_rope_hbm, gain_hbm, offsets, lat_out, rope_out = refs[:7]
    tok, w_own, w_rope, in_gain, normed = refs[7:12]
    wbuf, acc, own, transit = (refs[12 + k * groups : 12 + (k + 1) * groups] for k in range(4))
    (
        own_rope,
        transit_rope,
        local_sem,
        own_send,
        z_send,
        z_recv,
        a_send,
        a_recv,
        b_send,
        b_recv,
        c_send,
        c_recv,
        l_send,
        t_send,
        t_recv,
        x_send,
        e_send,
        d_send,
        l_recv,
    ) = refs[12 + 4 * groups :]
    n_x = n_tp // CORES
    prompts, rows = own[0].shape[:2]
    depth, cols = w_own.shape
    chunk = depth // (n_grp * n_tp)
    y, z, t = lax.axis_index("grp"), lax.axis_index("sp"), lax.axis_index("tp")
    x, core = t // CORES, t % CORES
    rank = (core * n_x + x) * n_grp + y

    def tp_of(x_to, core_to):
        return {"tp": x_to * CORES + core_to}

    partner = tp_of(x, 1 - core)
    x_peers = [lax.rem(x + k, n_x) for k in range(1, n_x)]
    y_peers = [lax.rem(y + k, n_grp) for k in range(1, n_grp)]
    z_up, z_down = lax.rem(z + 1, n_sp), lax.rem(z + n_sp - 1, n_sp)
    has_up, has_down = z + 1 < n_sp, z > 0

    fetch_tok = pltpu.make_async_copy(tok_hbm, tok, local_sem.at[0])
    fetch_w = pltpu.make_async_copy(w_hbm, w_own, local_sem.at[1])
    fetch_rope = pltpu.make_async_copy(w_rope_hbm, w_rope, local_sem.at[2])
    fetch_gain = pltpu.make_async_copy(gain_hbm, in_gain, local_sem.at[3])

    barrier = pltpu.get_barrier_semaphore()

    def greet(target):
        pl.semaphore_signal(barrier, inc=1, device_id=target, device_id_type=MESH)

    pl.when(has_up)(lambda: greet({"sp": z_up}))
    pl.when(has_down)(lambda: greet({"sp": z_down}))
    near = [tp_of(p, core) for p in x_peers] + [{"grp": p} for p in y_peers] + [partner]
    for target in near:
        greet(target)
    fetch_gain.start()
    fetch_tok.start()
    fetch_w.start()
    fetch_rope.start()
    pl.semaphore_wait(barrier, len(near) + has_up.astype(jnp.int32) + has_down.astype(jnp.int32))

    finish, fetched = [], []
    tuned = n_sp == 4 and groups == len(PARTS)
    doubled = DOUBLED if tuned and n_x == 2 and n_grp == 2 else (False,) * groups
    modes = MODES if tuned else ("F",) * (groups + 1)

    def remote(src, dst, send, recv, device):
        return pltpu.make_async_remote_copy(
            src_ref=src,
            dst_ref=dst,
            send_sem=send,
            recv_sem=recv,
            device_id=device,
            device_id_type=MESH,
        )

    def arrived(ref, recv):
        remote(ref, ref, recv, recv, partner).wait_recv()

    def need(copy):
        if not any(copy is other for other in fetched):
            fetched.append(copy)
            copy.wait()

    def begin(copy, when=None):
        if when is None:
            copy.start()
            finish.append(copy.wait_send)
        else:
            pl.when(when)(copy.start)
            finish.append(lambda: pl.when(when)(copy.wait_send))

    units = [(g, d) for g in range(groups) for d in range(1, n_sp)]
    above = n_sp - 1 - z
    both = jnp.minimum(z, above)

    def shard(d):
        paired = d <= 2 * both
        hop = jnp.where(paired, (d + 1) // 2, d - both)
        up = jnp.where(paired, d % 2 == 1, above > z)
        return jnp.where(up, z + hop, z - hop), up

    shards = {d: shard(d) for d in range(1, n_sp)}

    def corners(g):
        here = [(rank, x, y)]
        if doubled[g]:
            here.append(((core * n_x + 1 - x) * n_grp + 1 - y, 1 - x, 1 - y))
        return list(enumerate(here))

    def own_z(g):
        first, width = spans[g]
        for side, ahead, exists in ((0, z_up, has_up), (1, z_down, has_down)):
            for q, (index, at_x, at_y) in corners(g):
                copy = remote(
                    w_hbm.at[pl.ds(index * chunk, chunk), pl.ds(first, width)],
                    wbuf[g].at[z, core, at_x, at_y],
                    own_send.at[g, side, q],
                    z_recv.at[g, z, q],
                    {"sp": ahead},
                )
                begin(copy, exists)

    def x_first(u):
        return X_FIRST[u] if tuned else u % 4 > 0

    def spread(u, src, send, recv, along_x):
        peers = x_peers if along_x else y_peers
        for k, peer in enumerate(peers):
            device = tp_of(peer, core) if along_x else {"grp": peer}
            begin(remote(src, src, send.at[u, k], recv.at[u, k], device))

    def block_a(u):
        g, d = units[u]
        return wbuf[g].at[shards[d][0], core, x, y]

    def block_b(u):
        g, d = units[u]
        if x_first(u):
            return wbuf[g].at[shards[d][0], core, :, y]
        return wbuf[g].at[shards[d][0], core, x]

    def stage_z(u):
        g, d = units[u]
        s, up = shards[d]
        exists = jnp.where(up, has_down, has_up)
        ahead = jnp.where(up, z_down, z_up)
        for q, (_, at_x, at_y) in corners(g):
            block = wbuf[g].at[s, core, at_x, at_y]
            arrived(block, z_recv.at[g, s, q])
            begin(remote(block, block, z_send.at[u, q], z_recv.at[g, s, q], {"sp": ahead}), exists)

    def stage_a(u):
        if doubled[units[u][0]]:
            spread(u, block_a(u), a_send, a_recv, True)
            spread(u, block_a(u), b_send, b_recv, False)
        else:
            spread(u, block_a(u), a_send, a_recv, x_first(u))

    def stage_b(u):
        if doubled[units[u][0]]:
            return
        for k in range(len(x_peers if x_first(u) else y_peers)):
            arrived(block_a(u), a_recv.at[u, k])
        spread(u, block_b(u), b_send, b_recv, not x_first(u))

    def stage_c(u):
        g, d = units[u]
        if doubled[g]:
            arrived(block_a(u), a_recv.at[u, 0])
            arrived(block_a(u), b_recv.at[u, 0])
        else:
            for k in range(len(y_peers if x_first(u) else x_peers)):
                arrived(block_b(u), b_recv.at[u, k])
        ref = wbuf[g].at[shards[d][0], core]
        begin(remote(ref, ref, c_send.at[u], c_recv.at[u], partner))

    def stage_dot(u):
        g, d = units[u]
        s, _ = shards[d]
        arrived(wbuf[g].at[s, core], c_recv.at[u])
        weight = wbuf[g][s].reshape(depth, spans[g][1])
        acc[g][...] += jnp.dot(normed[s], weight, preferred_element_type=jnp.float32)

    def slot(m, s):
        if m == 0:
            return rope_out.at[s]
        first, width = spans[m - 1]
        return lat_out.at[s, :, pl.ds(first, width)]

    def mine(m, i):
        return own_rope.at[i] if m == 0 else own[m - 1].at[i]

    def held(m, k, i):
        return transit_rope.at[k, i] if m == 0 else transit[m - 1].at[k, i]

    def own_line(m, source, home):
        if modes[m] == "M":
            return (source + home + m) % 2 == 0
        return modes[m] == "O"

    def meet(first, second):
        if isinstance(second, bool):
            return first if second else None
        return first & second

    def stage_l(m):
        for i in range(prompts):
            home = t * prompts + i
            stays = leaves = True
            if modes[m] == "M":
                stays = own_line(m, z, home)
                leaves = jnp.logical_not(stays)
            elif modes[m] != "F":
                stays = own_line(m, z, home)
                leaves = not stays
            up_line = meet(home != z, stays)
            if up_line is not None:
                copy = remote(
                    mine(m, i), slot(m, z), l_send.at[m, i], l_recv.at[m, z], {"sp": home}
                )
                begin(copy, up_line)
            over = meet(home != z, leaves)
            for k, peer in enumerate(x_peers):
                device = tp_of(peer, core)
                beside = remote(mine(m, i), slot(m, z), x_send.at[m, i, k], l_recv.at[m, z], device)
                begin(beside, home == z)
                if over is not None:
                    across = remote(
                        mine(m, i), held(m, k, i), x_send.at[m, i, k], t_recv.at[m, k, i], device
                    )
                    begin(across, over)

    def stage_t(m):
        if modes[m] == "O":
            return
        for k in range(n_x - 1):
            source = lax.rem(x + n_x - 1 - k, n_x) * CORES + core
            for i in range(prompts):
                home = source * prompts + i
                comes = home != z
                if modes[m] == "M":
                    comes = comes & jnp.logical_not(own_line(m, z, home))
                copy = remote(
                    held(m, k, i), slot(m, z), t_send.at[m, k, i], l_recv.at[m, z], {"sp": home}
                )

                def pass_on(k=k, i=i, copy=copy):
                    arrived(held(m, k, i), t_recv.at[m, k, i])
                    copy.start()

                pl.when(comes)(pass_on)
                finish.append(lambda comes=comes, copy=copy: pl.when(comes)(copy.wait_send))

    owner = z // prompts
    x_in, core_in = owner // CORES, owner % CORES

    def partner_copy(m, d, s):
        return remote(slot(m, s), slot(m, s), d_send.at[m, d], l_recv.at[m, s], partner)

    def enters(m, d):
        here = core == core_in
        if d == 0 or modes[m] == "F":
            return here
        line = own_line(m, shards[d][0], z)
        if modes[m] == "M":
            return here & ((x == x_in) == line)
        return here & ((x == x_in) if line else (x != x_in))

    def stage_d(m, d):
        s = z if d == 0 else shards[d][0]
        copies = [partner_copy(m, d, s)]
        if d and modes[m] != "F":
            copies += [
                remote(slot(m, s), slot(m, s), e_send.at[m, d, k], l_recv.at[m, s], tp_of(peer, core))
                for k, peer in enumerate(x_peers)
            ]

        def hand():
            if d == 0:
                pl.when(x != x_in)(lambda: arrived(slot(m, s), l_recv.at[m, s]))
            else:
                arrived(slot(m, s), l_recv.at[m, s])
            for copy in reversed(copies):
                copy.start()

        def drain():
            for copy in copies:
                copy.wait_send()

        pl.when(enters(m, d))(hand)
        finish.append(lambda: pl.when(enters(m, d))(drain))

    def stage_e(m, d):
        s = shards[d][0]
        here = (core == core_in) & jnp.logical_not(enters(m, d))
        copy = partner_copy(m, d, s)

        def hand():
            arrived(slot(m, s), l_recv.at[m, s])
            copy.start()

        pl.when(here)(hand)
        finish.append(lambda: pl.when(here)(copy.wait_send))

    def stage_end(m, d):
        s = z if d == 0 else shards[d][0]
        pl.when(core != core_in)(lambda: arrived(slot(m, s), l_recv.at[m, s]))

    def finalize(m, values):
        for i in range(prompts):
            mine(m, i)[...] = values[i]

            def keep(i=i):
                slot(m, z)[...] = values[i]

            pl.when(t * prompts + i == z)(keep)

    step_rows, pieces = 16, PIECES

    def norm(r, carry):
        at = pl.ds(pl.multiple_of(r * step_rows, step_rows), step_rows)
        wide = tok[at, :].astype(jnp.float32)
        scale = lax.rsqrt(jnp.mean(wide * wide, axis=-1, keepdims=True) + EPS)
        out = (wide * scale * in_gain[...]).astype(jnp.bfloat16)
        for b in range(n_sp):
            normed[b, at, :] = out[:, b * depth : (b + 1) * depth]
        return carry

    def norm_piece(k):
        need(fetch_gain)
        need(fetch_tok)
        turns = prompts * rows // step_rows // pieces
        lax.fori_loop(k * turns, (k + 1) * turns, norm, 0)

    def own_dot(g):
        first, width = spans[g]
        need(fetch_w)
        acc[g][...] = jnp.dot(
            normed[z], w_own[:, first : first + width], preferred_element_type=jnp.float32
        )

    def rope_item():
        need(fetch_rope)
        raw = jnp.zeros((ROPE, prompts * rows), jnp.float32)
        for b in range(n_sp):
            raw += lax.dot_general(
                w_rope[:, b * depth : (b + 1) * depth],
                normed[b],
                (((1,), (1,)), ((), ())),
                preferred_element_type=jnp.float32,
            )
        half = ROPE // 2
        index = lax.broadcasted_iota(jnp.int32, (half, rows), 1)
        channel = lax.broadcasted_iota(jnp.int32, (half, rows), 0)
        inverse = jnp.zeros((half, rows), jnp.float32)
        for c, value in enumerate(frequency):
            inverse = jnp.where(channel == c, value, inverse)
        values = []
        for i in range(prompts):
            position = offsets[i] + z * rows + index
            angle = position.astype(jnp.float32) * inverse
            sine, cosine = jnp.sin(angle), jnp.cos(angle)
            first = raw[:half, i * rows : (i + 1) * rows]
            second = raw[half:, i * rows : (i + 1) * rows]
            turned = [first * cosine - second * sine, second * cosine + first * sine]
            values.append(jnp.concatenate(turned, axis=0).astype(jnp.bfloat16))
        finalize(0, values)

    def group_item(g):
        value = acc[g][...].astype(jnp.bfloat16)
        finalize(g + 1, [value[i * rows : (i + 1) * rows] for i in range(prompts)])

    def latent_item(m):
        if m == 0:
            rope_item()
        else:
            group_item(m - 1)
        stage_l(m)

    stages = {
        "own": own_z,
        "norm": norm_piece,
        "odot": own_dot,
        "z": stage_z,
        "a": stage_a,
        "b": stage_b,
        "c": stage_c,
        "dot": stage_dot,
        "l": latent_item,
        "t": stage_t,
        "d": stage_d,
        "e": stage_e,
        "end": stage_end,
    }

    def run(schedule, middle):
        finish.clear()
        fetched.clear()
        for name, *args in schedule:
            if name == "a" and not middle:
                stage_z(*args)
            stages[name](*args)
            while len(finish) > PENDING:
                finish.pop(0)()
        for fn in finish:
            fn()

    if tuned:
        inner = has_up & has_down
        pl.when(inner)(lambda: run(MIDDLE, True))
        pl.when(jnp.logical_not(inner))(lambda: run(OUTER, False))
    else:
        run(plain_schedule(units, groups, n_sp), False)


def gather_latent(tokens, w_latent, w_rope, in_gain, offsets, frequency):
    prompts, rows, width = tokens.shape
    n_grp, n_sp, n_tp = (lax.axis_size(a) for a in ("grp", "sp", "tp"))
    n_x = n_tp // CORES
    depth, cols = w_latent.shape
    spans = column_groups(n_sp, cols)
    groups = len(spans)
    chunk = depth // (n_grp * n_tp)
    total = prompts * rows
    units = groups * (n_sp - 1)
    peers = max(n_x, n_grp) - 1
    others = max(n_x - 1, 1)
    items = groups + 1
    bf16, f32 = jnp.bfloat16, jnp.float32
    dma = pltpu.SemaphoreType.DMA
    stay = lambda a: pltpu.with_memory_space_constraint(a, pltpu.HBM)
    limit = (40 if groups > 1 else 60) * 1024 * 1024
    vmem = pl.BlockSpec(memory_space=pltpu.VMEM)
    hbm = pl.BlockSpec(memory_space=pltpu.HBM)
    return pl.pallas_call(
        functools.partial(gather_kernel, n_grp, n_sp, n_tp, spans, frequency),
        out_shape=(
            jax.ShapeDtypeStruct((n_sp, rows, cols), bf16),
            jax.ShapeDtypeStruct((n_sp, ROPE, rows), bf16),
        ),
        in_specs=[hbm, hbm, hbm, hbm, pl.BlockSpec(memory_space=pltpu.SMEM)],
        out_specs=(vmem, vmem),
        scratch_shapes=[
            pltpu.VMEM((total, width), bf16),
            pltpu.VMEM((depth, cols), bf16),
            pltpu.VMEM((ROPE, width), bf16),
            pltpu.VMEM((1, width), f32),
            pltpu.VMEM((n_sp, total, depth), bf16),
            *[pltpu.VMEM((n_sp, CORES, n_x, n_grp, chunk, w), bf16) for _, w in spans],
            *[pltpu.VMEM((total, w), f32) for _, w in spans],
            *[pltpu.VMEM((prompts, rows, w), bf16) for _, w in spans],
            *[pltpu.VMEM((others, prompts, rows, w), bf16) for _, w in spans],
            pltpu.VMEM((prompts, ROPE, rows), bf16),
            pltpu.VMEM((others, prompts, ROPE, rows), bf16),
            dma((4,)),
            dma((groups, 2, 2)),
            dma((units, 2)),
            dma((groups, n_sp, 2)),
            dma((units, peers)),
            dma((units, peers)),
            dma((units, peers)),
            dma((units, peers)),
            dma((units,)),
            dma((units,)),
            dma((items, prompts)),
            dma((items, others, prompts)),
            dma((items, others, prompts)),
            dma((items, prompts, others)),
            dma((items, n_sp, others)),
            dma((items, n_sp)),
            dma((items, n_sp)),
        ],
        compiler_params=pltpu.CompilerParams(
            collective_id=0, has_side_effects=True, vmem_limit_bytes=limit
        ),
    )(*map(stay, (tokens.reshape(total, width), w_latent, w_rope, in_gain)), offsets)


def cache_kernel(
    latent_ref,
    gain_ref,
    wk_ref,
    wv_ref,
    q_nope_ref,
    q_rope_ref,
    rope_ref,
    keys_hbm,
    values_hbm,
    rope_keys_ref,
    read_ref,
    latents,
    keys,
    values,
    sems,
):
    n_blocks, rows, out_cols = keys.shape
    heads = out_cols // HEAD

    def per_head(row, size):
        wide = jnp.broadcast_to(row.astype(jnp.float32), (heads, heads * size))
        head = lax.broadcasted_iota(jnp.int32, wide.shape, 0)
        lane = lax.broadcasted_iota(jnp.int32, wide.shape, 1)
        return jnp.where((lane >= head * size) & (lane < head * size + size), wide, 0.0)

    def put(b, source, target, kind):
        copy = pltpu.make_async_copy(
            source.at[b], target.at[pl.ds(b * rows, rows), :], sems.at[kind, b]
        )
        copy.start()
        return copy

    query = per_head(q_nope_ref[...], HEAD).astype(jnp.bfloat16)
    spread = (heads * ROPE, ROPE)
    fold = lax.broadcasted_iota(jnp.int32, spread, 0) % ROPE == lax.broadcasted_iota(
        jnp.int32, spread, 1
    )
    rotary_q = jnp.dot(
        per_head(q_rope_ref[...], ROPE).astype(jnp.bfloat16),
        jnp.where(fold, 1.0, 0.0).astype(jnp.bfloat16),
        preferred_element_type=jnp.float32,
    ).astype(jnp.bfloat16)
    across = (((1,), (1,)), ((), ()))
    copies, scores = [], []

    def normalize(b):
        raw = latent_ref[b].astype(jnp.float32)
        scale = lax.rsqrt(jnp.mean(raw * raw, axis=-1, keepdims=True) + EPS)
        latents[b] = (raw * scale * gain_ref[...]).astype(jnp.bfloat16)

    def up_key(b):
        block = jnp.dot(latents[b], wk_ref[...], preferred_element_type=jnp.float32)
        keys[b] = block.astype(jnp.bfloat16)
        copies.append(put(b, keys, keys_hbm, 0))

    def up_value(b):
        block = jnp.dot(latents[b], wv_ref[...], preferred_element_type=jnp.float32)
        values[b] = block.astype(jnp.bfloat16)
        copies.append(put(b, values, values_hbm, 1))

    def score(b):
        part = lax.dot_general(query, keys[b], across, preferred_element_type=jnp.float32)
        part += jnp.dot(rotary_q, rope_ref[b], preferred_element_type=jnp.float32)
        scores.append(part / jnp.sqrt(jnp.float32(HEAD + ROPE)))
        rope_keys_ref[:, b * rows : (b + 1) * rows] = rope_ref[b]

    normalize(0)
    for b in range(n_blocks):
        if b + 1 < n_blocks:
            normalize(b + 1)
        up_key(b)
        if b + 1 < n_blocks:
            up_value(b)
        score(b)
    up_value(n_blocks - 1)
    peak = functools.reduce(jnp.maximum, scores).max(axis=-1, keepdims=True)
    expos = [jnp.exp(part - peak) for part in scores]
    total = functools.reduce(jnp.add, expos).sum(axis=-1, keepdims=True)
    out = jnp.zeros((heads, out_cols), jnp.float32)
    for b in range(n_blocks):
        weights = (expos[b] / total).astype(jnp.bfloat16)
        out += jnp.dot(weights, values[b], preferred_element_type=jnp.float32)
    head = lax.broadcasted_iota(jnp.int32, out.shape, 0)
    lane = lax.broadcasted_iota(jnp.int32, out.shape, 1)
    picked = jnp.where((lane >= head * HEAD) & (lane < head * HEAD + HEAD), out, 0.0)
    read_ref[...] = jnp.sum(picked, axis=0, keepdims=True).astype(jnp.bfloat16)
    for copy in copies:
        copy.wait()


def fill_cache(latent, kv_gain, w_up_key, w_up_value, q_nope, q_rope, rope):
    n_blocks, rows, cols = latent.shape
    out_cols = w_up_key.shape[1]
    length = n_blocks * rows
    vmem = pl.BlockSpec(memory_space=pltpu.VMEM)
    hbm = pl.BlockSpec(memory_space=pltpu.HBM)
    return pl.pallas_call(
        cache_kernel,
        out_shape=(
            jax.ShapeDtypeStruct((length, out_cols), jnp.bfloat16),
            jax.ShapeDtypeStruct((length, out_cols), jnp.bfloat16),
            jax.ShapeDtypeStruct((ROPE, length), jnp.bfloat16),
            jax.ShapeDtypeStruct((1, out_cols), jnp.bfloat16),
        ),
        in_specs=[vmem] * 7,
        out_specs=(hbm, hbm, vmem, vmem),
        scratch_shapes=[
            pltpu.VMEM((n_blocks, rows, cols), jnp.bfloat16),
            pltpu.VMEM((n_blocks, rows, out_cols), jnp.bfloat16),
            pltpu.VMEM((n_blocks, rows, out_cols), jnp.bfloat16),
            pltpu.SemaphoreType.DMA((2, n_blocks)),
        ],
        compiler_params=pltpu.CompilerParams(vmem_limit_bytes=40 * 1024 * 1024),
    )(latent, kv_gain, w_up_key, w_up_value, q_nope, q_rope, rope)


def local(
    tokens, offsets, in_gain, w_latent, w_rope_key, kv_gain, w_up_key, w_up_value, q_nope, q_rope
):
    steps = -np.arange(0, ROPE, 2).astype(np.float32) / ROPE
    frequency = [float(f) for f in np.float32(10000.0) ** steps]
    latent, rope = gather_latent(tokens, w_latent, w_rope_key.T, in_gain[None], offsets, frequency)
    keys, values, rope_keys, read = fill_cache(
        latent, kv_gain[None], w_up_key, w_up_value, q_nope, q_rope, rope
    )
    return (keys[None], values[None], rope_keys[None], read)


def solution(mesh):
    in_specs = (
        P(("grp", "tp"), "sp", None),
        P(("grp", "tp")),
        P(),
        P("sp", None),
        P(),
        P(),
        P(None, "tp"),
        P(None, "tp"),
        P(("grp", "sp"), "tp"),
        P(("grp", "sp"), "tp"),
    )
    out_specs = (
        P(("grp", "sp"), None, "tp"),
        P(("grp", "sp"), None, "tp"),
        P(("grp", "sp"), None, None),
        P(("grp", "sp"), "tp"),
    )
    return jax.shard_map(local, mesh=mesh, in_specs=in_specs, out_specs=out_specs, check_vma=False)
```

```python
import functools

import jax
import jax.numpy as jnp
import numpy as np
from jax import lax
from jax.experimental import pallas as pl
from jax.experimental.pallas import tpu as pltpu
from jax.sharding import PartitionSpec as P

HEAD = 64
ROPE = 32
CORES = 2
PIECES = 4
PENDING = 60
PARTS = (1, 1, 1, 1, 1, 1, 1, 1)
MODES = ("M", "C", "C", "O", "O", "C", "C", "O", "O")
DOUBLED = (False, False, False, False, True, True, True, True)
X_FIRST = (True, False, True, False, True, True, True, False, False, True, True, True, True, False, False, True, True, True, False, False, False, False, False, False)
OUTER = (
    ("own", 0), ("norm", 0), ("own", 1), ("norm", 1), ("norm", 2), ("own", 2), ("norm", 3),
    ("odot", 0), ("odot", 1), ("odot", 2), ("odot", 4), ("odot", 6), ("own", 3), ("odot", 5),
    ("odot", 7), ("odot", 3), ("a", 3), ("a", 0), ("a", 6), ("own", 5), ("a", 1), ("b", 0),
    ("a", 9), ("own", 4), ("b", 6), ("b", 3), ("a", 4), ("a", 7), ("c", 0), ("a", 2), ("b", 9),
    ("b", 1), ("a", 12), ("b", 12), ("l", 0), ("a", 5), ("a", 10), ("own", 6), ("c", 6), ("b", 4),
    ("dot", 0), ("a", 8), ("dot", 6), ("b", 7), ("a", 15), ("c", 1), ("b", 2), ("own", 7),
    ("a", 18), ("b", 18), ("c", 12), ("c", 3), ("a", 13), ("b", 5), ("dot", 3), ("t", 0),
    ("dot", 12), ("c", 4), ("c", 9), ("b", 10), ("dot", 1), ("b", 8), ("a", 16), ("c", 2),
    ("dot", 9), ("a", 11), ("b", 13), ("c", 7), ("dot", 7), ("c", 13), ("a", 21), ("a", 14),
    ("b", 14), ("dot", 2), ("l", 1), ("d", 0, 2), ("a", 19), ("b", 15), ("c", 15), ("dot", 4),
    ("c", 18), ("c", 5), ("dot", 13), ("d", 0, 0), ("b", 16), ("c", 16), ("b", 11), ("c", 10),
    ("c", 8), ("dot", 18), ("a", 22), ("b", 22), ("dot", 5), ("l", 2), ("a", 17), ("dot", 10),
    ("d", 0, 3), ("dot", 8), ("l", 3), ("c", 14), ("dot", 16), ("d", 0, 1), ("a", 20), ("b", 20),
    ("dot", 15), ("t", 1), ("d", 1, 0), ("a", 23), ("c", 11), ("b", 19), ("c", 19), ("c", 22),
    ("dot", 14), ("l", 5), ("dot", 11), ("l", 4), ("b", 23), ("dot", 19), ("t", 2), ("b", 17),
    ("c", 17), ("d", 2, 0), ("dot", 22), ("b", 21), ("c", 21), ("e", 0, 2), ("e", 0, 3),
    ("dot", 17), ("l", 6), ("d", 1, 2), ("c", 20), ("dot", 21), ("e", 0, 1), ("c", 23), ("d", 3, 0),
    ("d", 1, 3), ("d", 4, 0), ("d", 3, 1), ("d", 3, 2), ("dot", 20), ("l", 7), ("d", 3, 3),
    ("d", 2, 3), ("t", 5), ("d", 5, 0), ("d", 5, 1), ("d", 5, 2), ("dot", 23), ("l", 8),
    ("d", 8, 1), ("d", 2, 1), ("d", 7, 2), ("d", 2, 2), ("e", 2, 3), ("t", 6), ("d", 6, 0),
    ("d", 7, 1), ("d", 4, 3), ("d", 1, 1), ("e", 1, 2), ("d", 6, 1), ("d", 5, 3), ("e", 5, 2),
    ("d", 6, 2), ("d", 4, 2), ("d", 4, 1), ("e", 3, 2), ("e", 5, 1), ("d", 6, 3), ("e", 3, 1),
    ("d", 7, 0), ("e", 3, 3), ("e", 2, 1), ("e", 1, 3), ("e", 2, 2), ("d", 8, 0), ("d", 7, 3),
    ("e", 7, 2), ("e", 4, 2), ("e", 4, 1), ("e", 7, 1), ("d", 8, 2), ("d", 8, 3), ("e", 1, 1),
    ("e", 6, 1), ("e", 4, 3), ("e", 5, 3), ("e", 8, 1), ("e", 7, 3), ("e", 6, 2), ("e", 8, 2),
    ("e", 8, 3), ("e", 6, 3), ("end", 0, 0), ("end", 0, 1), ("end", 0, 2), ("end", 0, 3),
    ("end", 1, 0), ("end", 1, 1), ("end", 1, 2), ("end", 1, 3), ("end", 2, 0), ("end", 2, 1),
    ("end", 2, 2), ("end", 2, 3), ("end", 3, 0), ("end", 3, 1), ("end", 3, 2), ("end", 3, 3),
    ("end", 4, 0), ("end", 4, 1), ("end", 4, 2), ("end", 4, 3), ("end", 5, 0), ("end", 5, 1),
    ("end", 5, 2), ("end", 5, 3), ("end", 6, 0), ("end", 6, 1), ("end", 6, 2), ("end", 6, 3),
    ("end", 7, 0), ("end", 7, 1), ("end", 7, 2), ("end", 7, 3), ("end", 8, 0), ("end", 8, 1),
    ("end", 8, 2), ("end", 8, 3),
)
MIDDLE = (
    ("own", 1), ("norm", 1), ("own", 0), ("norm", 0), ("own", 2), ("norm", 2), ("norm", 3),
    ("z", 0), ("z", 1), ("a", 0), ("z", 4), ("own", 3), ("odot", 1), ("a", 1), ("odot", 0),
    ("odot", 2), ("odot", 3), ("a", 4), ("z", 3), ("odot", 5), ("odot", 6), ("odot", 7),
    ("odot", 4), ("own", 4), ("a", 3), ("b", 0), ("z", 7), ("a", 7), ("z", 6), ("z", 2), ("a", 2),
    ("l", 0), ("b", 1), ("z", 10), ("z", 9), ("z", 5), ("b", 4), ("own", 5), ("a", 6), ("z", 8),
    ("a", 8), ("a", 10), ("b", 3), ("b", 2), ("c", 0), ("a", 5), ("a", 9), ("b", 7), ("own", 6),
    ("z", 13), ("z", 16), ("a", 13), ("b", 13), ("b", 10), ("z", 11), ("z", 12), ("a", 12),
    ("b", 12), ("b", 6), ("z", 15), ("a", 15), ("b", 15), ("own", 7), ("c", 4), ("c", 1),
    ("dot", 1), ("z", 14), ("z", 18), ("a", 18), ("c", 13), ("b", 8), ("dot", 0), ("z", 19),
    ("b", 5), ("c", 3), ("c", 2), ("a", 11), ("a", 16), ("b", 16), ("c", 15), ("b", 9), ("dot", 4),
    ("z", 22), ("b", 18), ("c", 7), ("c", 12), ("a", 14), ("c", 6), ("a", 22), ("dot", 3),
    ("dot", 2), ("l", 1), ("z", 21), ("c", 18), ("dot", 18), ("a", 19), ("b", 19), ("t", 0),
    ("c", 10), ("z", 17), ("z", 20), ("a", 17), ("b", 17), ("dot", 7), ("d", 0, 0), ("a", 21),
    ("b", 21), ("dot", 12), ("c", 5), ("c", 16), ("b", 22), ("b", 11), ("dot", 13), ("b", 14),
    ("a", 20), ("b", 20), ("dot", 15), ("c", 14), ("z", 23), ("c", 9), ("dot", 9), ("c", 22),
    ("a", 23), ("b", 23), ("c", 8), ("dot", 5), ("l", 2), ("t", 1), ("d", 1, 0), ("c", 17),
    ("c", 19), ("dot", 22), ("c", 21), ("dot", 14), ("l", 5), ("dot", 10), ("dot", 16), ("dot", 6),
    ("c", 20), ("c", 11), ("dot", 8), ("l", 3), ("dot", 17), ("l", 6), ("d", 1, 1), ("c", 23),
    ("d", 3, 0), ("d", 1, 2), ("dot", 20), ("dot", 19), ("l", 7), ("d", 1, 3), ("dot", 21),
    ("dot", 11), ("l", 4), ("d", 0, 2), ("d", 0, 1), ("t", 5), ("d", 5, 0), ("d", 0, 3),
    ("e", 0, 3), ("dot", 23), ("l", 8), ("t", 2), ("d", 2, 0), ("d", 2, 3), ("d", 3, 2),
    ("d", 2, 1), ("t", 6), ("d", 3, 1), ("d", 3, 3), ("d", 4, 0), ("e", 3, 3), ("e", 1, 1),
    ("e", 1, 2), ("d", 7, 0), ("d", 2, 2), ("d", 6, 0), ("d", 4, 3), ("d", 7, 2), ("d", 4, 2),
    ("e", 2, 3), ("d", 4, 1), ("d", 7, 3), ("e", 0, 2), ("d", 7, 1), ("e", 3, 1), ("d", 5, 2),
    ("e", 3, 2), ("e", 4, 3), ("d", 5, 1), ("d", 8, 0), ("e", 7, 2), ("e", 2, 2), ("d", 5, 3),
    ("e", 1, 3), ("d", 8, 3), ("d", 6, 2), ("d", 8, 2), ("d", 8, 1), ("e", 4, 2), ("e", 2, 1),
    ("e", 4, 1), ("e", 5, 3), ("e", 0, 1), ("d", 6, 1), ("e", 5, 2), ("d", 6, 3), ("e", 6, 2),
    ("e", 6, 1), ("e", 7, 3), ("e", 7, 1), ("e", 5, 1), ("e", 8, 3), ("e", 6, 3), ("e", 8, 2),
    ("e", 8, 1), ("end", 0, 0), ("end", 0, 1), ("end", 0, 2), ("end", 0, 3), ("end", 1, 0),
    ("end", 1, 1), ("end", 1, 2), ("end", 1, 3), ("end", 2, 0), ("end", 2, 1), ("end", 2, 2),
    ("end", 2, 3), ("end", 3, 0), ("end", 3, 1), ("end", 3, 2), ("end", 3, 3), ("end", 4, 0),
    ("end", 4, 1), ("end", 4, 2), ("end", 4, 3), ("end", 5, 0), ("end", 5, 1), ("end", 5, 2),
    ("end", 5, 3), ("end", 6, 0), ("end", 6, 1), ("end", 6, 2), ("end", 6, 3), ("end", 7, 0),
    ("end", 7, 1), ("end", 7, 2), ("end", 7, 3), ("end", 8, 0), ("end", 8, 1), ("end", 8, 2),
    ("end", 8, 3),
)

EPS = 1e-06
MESH = pl.DeviceIdType.MESH


def column_groups(n_sp, cols):
    if n_sp > 4 or cols % 1024:
        return [(0, cols)]
    each, total, out = cols // sum(PARTS), 0, []
    for part in PARTS:
        out.append((total, part * each))
        total += part * each
    return out


def plain_schedule(units, groups, n_sp):
    late = len(units) * 10
    ops = [(g, ("own", g)) for g in range(groups)]
    ops += [(k, ("norm", k)) for k in range(PIECES)]
    ops += [(PIECES + g, ("odot", g)) for g in range(groups)]
    done = {}
    for u, (g, d) in enumerate(units):
        at = PIECES + 2 + u
        ops += [(at, ("a", u)), (at + 2, ("b", u)), (at + 4, ("c", u)), (at + 5, ("dot", u))]
        done[g + 1] = at + 5
    for m in range(groups + 1):
        at = done.get(m, PIECES + 1)
        ops += [(at + 0.5, ("l", m)), (at + 3, ("t", m))]
        ops += [(at + 6, ("d", m, d)) for d in range(n_sp)]
        ops += [(late + m, ("end", m, d)) for d in range(n_sp)]
    return [op for _, op in sorted(ops, key=lambda item: item[0])]


def gather_kernel(n_grp, n_sp, n_tp, spans, frequency, *refs):
    groups = len(spans)
    tok_hbm, w_hbm, w_rope_hbm, gain_hbm, offsets, lat_out, rope_out = refs[:7]
    tok, w_own, w_rope, in_gain, normed = refs[7:12]
    wbuf, acc, own, transit = (refs[12 + k * groups : 12 + (k + 1) * groups] for k in range(4))
    (
        own_rope,
        transit_rope,
        local_sem,
        own_send,
        z_send,
        z_recv,
        a_send,
        a_recv,
        b_send,
        b_recv,
        c_send,
        c_recv,
        l_send,
        t_send,
        t_recv,
        x_send,
        e_send,
        d_send,
        l_recv,
    ) = refs[12 + 4 * groups :]
    n_x = n_tp // CORES
    prompts, rows = own[0].shape[:2]
    depth, cols = w_own.shape
    chunk = depth // (n_grp * n_tp)
    y, z, t = lax.axis_index("grp"), lax.axis_index("sp"), lax.axis_index("tp")
    x, core = t // CORES, t % CORES
    rank = (core * n_x + x) * n_grp + y

    def tp_of(x_to, core_to):
        return {"tp": x_to * CORES + core_to}

    partner = tp_of(x, 1 - core)
    x_peers = [lax.rem(x + k, n_x) for k in range(1, n_x)]
    y_peers = [lax.rem(y + k, n_grp) for k in range(1, n_grp)]
    z_up, z_down = lax.rem(z + 1, n_sp), lax.rem(z + n_sp - 1, n_sp)
    has_up, has_down = z + 1 < n_sp, z > 0

    fetch_tok = pltpu.make_async_copy(tok_hbm, tok, local_sem.at[0])
    fetch_w = pltpu.make_async_copy(w_hbm, w_own, local_sem.at[1])
    fetch_rope = pltpu.make_async_copy(w_rope_hbm, w_rope, local_sem.at[2])
    fetch_gain = pltpu.make_async_copy(gain_hbm, in_gain, local_sem.at[3])

    barrier = pltpu.get_barrier_semaphore()

    def greet(target):
        pl.semaphore_signal(barrier, inc=1, device_id=target, device_id_type=MESH)

    pl.when(has_up)(lambda: greet({"sp": z_up}))
    pl.when(has_down)(lambda: greet({"sp": z_down}))
    near = [tp_of(p, core) for p in x_peers] + [{"grp": p} for p in y_peers] + [partner]
    for target in near:
        greet(target)
    fetch_gain.start()
    fetch_tok.start()
    fetch_w.start()
    fetch_rope.start()
    pl.semaphore_wait(barrier, len(near) + has_up.astype(jnp.int32) + has_down.astype(jnp.int32))

    finish, fetched = [], []
    tuned = n_sp == 4 and groups == len(PARTS)
    doubled = DOUBLED if tuned and n_x == 2 and n_grp == 2 else (False,) * groups
    modes = MODES if tuned else ("F",) * (groups + 1)

    def remote(src, dst, send, recv, device):
        return pltpu.make_async_remote_copy(
            src_ref=src,
            dst_ref=dst,
            send_sem=send,
            recv_sem=recv,
            device_id=device,
            device_id_type=MESH,
        )

    def arrived(ref, recv):
        remote(ref, ref, recv, recv, partner).wait_recv()

    def need(copy):
        if not any(copy is other for other in fetched):
            fetched.append(copy)
            copy.wait()

    def begin(copy, when=None):
        if when is None:
            copy.start()
            finish.append(copy.wait_send)
        else:
            pl.when(when)(copy.start)
            finish.append(lambda: pl.when(when)(copy.wait_send))

    units = [(g, d) for g in range(groups) for d in range(1, n_sp)]
    above = n_sp - 1 - z
    both = jnp.minimum(z, above)

    def shard(d):
        paired = d <= 2 * both
        hop = jnp.where(paired, (d + 1) // 2, d - both)
        up = jnp.where(paired, d % 2 == 1, above > z)
        return jnp.where(up, z + hop, z - hop), up

    shards = {d: shard(d) for d in range(1, n_sp)}

    def corners(g):
        here = [(rank, x, y)]
        if doubled[g]:
            here.append(((core * n_x + 1 - x) * n_grp + 1 - y, 1 - x, 1 - y))
        return list(enumerate(here))

    def own_z(g):
        first, width = spans[g]
        for side, ahead, exists in ((0, z_up, has_up), (1, z_down, has_down)):
            for q, (index, at_x, at_y) in corners(g):
                copy = remote(
                    w_hbm.at[pl.ds(index * chunk, chunk), pl.ds(first, width)],
                    wbuf[g].at[z, core, at_x, at_y],
                    own_send.at[g, side, q],
                    z_recv.at[g, z, q],
                    {"sp": ahead},
                )
                begin(copy, exists)

    def x_first(u):
        return X_FIRST[u] if tuned else u % 4 > 0

    def spread(u, src, send, recv, along_x):
        peers = x_peers if along_x else y_peers
        for k, peer in enumerate(peers):
            device = tp_of(peer, core) if along_x else {"grp": peer}
            begin(remote(src, src, send.at[u, k], recv.at[u, k], device))

    def block_a(u):
        g, d = units[u]
        return wbuf[g].at[shards[d][0], core, x, y]

    def block_b(u):
        g, d = units[u]
        if x_first(u):
            return wbuf[g].at[shards[d][0], core, :, y]
        return wbuf[g].at[shards[d][0], core, x]

    def stage_z(u):
        g, d = units[u]
        s, up = shards[d]
        exists = jnp.where(up, has_down, has_up)
        ahead = jnp.where(up, z_down, z_up)
        for q, (_, at_x, at_y) in corners(g):
            block = wbuf[g].at[s, core, at_x, at_y]
            arrived(block, z_recv.at[g, s, q])
            begin(remote(block, block, z_send.at[u, q], z_recv.at[g, s, q], {"sp": ahead}), exists)

    def stage_a(u):
        if doubled[units[u][0]]:
            spread(u, block_a(u), a_send, a_recv, True)
            spread(u, block_a(u), b_send, b_recv, False)
        else:
            spread(u, block_a(u), a_send, a_recv, x_first(u))

    def stage_b(u):
        if doubled[units[u][0]]:
            return
        for k in range(len(x_peers if x_first(u) else y_peers)):
            arrived(block_a(u), a_recv.at[u, k])
        spread(u, block_b(u), b_send, b_recv, not x_first(u))

    def stage_c(u):
        g, d = units[u]
        if doubled[g]:
            arrived(block_a(u), a_recv.at[u, 0])
            arrived(block_a(u), b_recv.at[u, 0])
        else:
            for k in range(len(y_peers if x_first(u) else x_peers)):
                arrived(block_b(u), b_recv.at[u, k])
        ref = wbuf[g].at[shards[d][0], core]
        begin(remote(ref, ref, c_send.at[u], c_recv.at[u], partner))

    def stage_dot(u):
        g, d = units[u]
        s, _ = shards[d]
        arrived(wbuf[g].at[s, core], c_recv.at[u])
        weight = wbuf[g][s].reshape(depth, spans[g][1])
        acc[g][...] += jnp.dot(normed[s], weight, preferred_element_type=jnp.float32)

    def slot(m, s):
        if m == 0:
            return rope_out.at[s]
        first, width = spans[m - 1]
        return lat_out.at[s, :, pl.ds(first, width)]

    def mine(m, i):
        return own_rope.at[i] if m == 0 else own[m - 1].at[i]

    def held(m, k, i):
        return transit_rope.at[k, i] if m == 0 else transit[m - 1].at[k, i]

    def own_line(m, source, home):
        if modes[m] == "M":
            return (source + home + m) % 2 == 0
        return modes[m] == "O"

    def meet(first, second):
        if isinstance(second, bool):
            return first if second else None
        return first & second

    def stage_l(m):
        for i in range(prompts):
            home = t * prompts + i
            stays = leaves = True
            if modes[m] == "M":
                stays = own_line(m, z, home)
                leaves = jnp.logical_not(stays)
            elif modes[m] != "F":
                stays = own_line(m, z, home)
                leaves = not stays
            up_line = meet(home != z, stays)
            if up_line is not None:
                copy = remote(
                    mine(m, i), slot(m, z), l_send.at[m, i], l_recv.at[m, z], {"sp": home}
                )
                begin(copy, up_line)
            over = meet(home != z, leaves)
            for k, peer in enumerate(x_peers):
                device = tp_of(peer, core)
                beside = remote(mine(m, i), slot(m, z), x_send.at[m, i, k], l_recv.at[m, z], device)
                begin(beside, home == z)
                if over is not None:
                    across = remote(
                        mine(m, i), held(m, k, i), x_send.at[m, i, k], t_recv.at[m, k, i], device
                    )
                    begin(across, over)

    def stage_t(m):
        if modes[m] == "O":
            return
        for k in range(n_x - 1):
            source = lax.rem(x + n_x - 1 - k, n_x) * CORES + core
            for i in range(prompts):
                home = source * prompts + i
                comes = home != z
                if modes[m] == "M":
                    comes = comes & jnp.logical_not(own_line(m, z, home))
                copy = remote(
                    held(m, k, i), slot(m, z), t_send.at[m, k, i], l_recv.at[m, z], {"sp": home}
                )

                def pass_on(k=k, i=i, copy=copy):
                    arrived(held(m, k, i), t_recv.at[m, k, i])
                    copy.start()

                pl.when(comes)(pass_on)
                finish.append(lambda comes=comes, copy=copy: pl.when(comes)(copy.wait_send))

    owner = z // prompts
    x_in, core_in = owner // CORES, owner % CORES

    def partner_copy(m, d, s):
        return remote(slot(m, s), slot(m, s), d_send.at[m, d], l_recv.at[m, s], partner)

    def enters(m, d):
        here = core == core_in
        if d == 0 or modes[m] == "F":
            return here
        line = own_line(m, shards[d][0], z)
        if modes[m] == "M":
            return here & ((x == x_in) == line)
        return here & ((x == x_in) if line else (x != x_in))

    def stage_d(m, d):
        s = z if d == 0 else shards[d][0]
        copies = [partner_copy(m, d, s)]
        if d and modes[m] != "F":
            copies += [
                remote(slot(m, s), slot(m, s), e_send.at[m, d, k], l_recv.at[m, s], tp_of(peer, core))
                for k, peer in enumerate(x_peers)
            ]

        def hand():
            if d == 0:
                pl.when(x != x_in)(lambda: arrived(slot(m, s), l_recv.at[m, s]))
            else:
                arrived(slot(m, s), l_recv.at[m, s])
            for copy in reversed(copies):
                copy.start()

        def drain():
            for copy in copies:
                copy.wait_send()

        pl.when(enters(m, d))(hand)
        finish.append(lambda: pl.when(enters(m, d))(drain))

    def stage_e(m, d):
        s = shards[d][0]
        here = (core == core_in) & jnp.logical_not(enters(m, d))
        copy = partner_copy(m, d, s)

        def hand():
            arrived(slot(m, s), l_recv.at[m, s])
            copy.start()

        pl.when(here)(hand)
        finish.append(lambda: pl.when(here)(copy.wait_send))

    def stage_end(m, d):
        s = z if d == 0 else shards[d][0]
        pl.when(core != core_in)(lambda: arrived(slot(m, s), l_recv.at[m, s]))

    def finalize(m, values):
        for i in range(prompts):
            mine(m, i)[...] = values[i]

            def keep(i=i):
                slot(m, z)[...] = values[i]

            pl.when(t * prompts + i == z)(keep)

    step_rows, pieces = 16, PIECES

    def norm(r, carry):
        at = pl.ds(pl.multiple_of(r * step_rows, step_rows), step_rows)
        wide = tok[at, :].astype(jnp.float32)
        scale = lax.rsqrt(jnp.mean(wide * wide, axis=-1, keepdims=True) + EPS)
        out = (wide * scale * in_gain[...]).astype(jnp.bfloat16)
        for b in range(n_sp):
            normed[b, at, :] = out[:, b * depth : (b + 1) * depth]
        return carry

    def norm_piece(k):
        need(fetch_gain)
        need(fetch_tok)
        turns = prompts * rows // step_rows // pieces
        lax.fori_loop(k * turns, (k + 1) * turns, norm, 0)

    def own_dot(g):
        first, width = spans[g]
        need(fetch_w)
        acc[g][...] = jnp.dot(
            normed[z], w_own[:, first : first + width], preferred_element_type=jnp.float32
        )

    def rope_item():
        need(fetch_rope)
        raw = jnp.zeros((ROPE, prompts * rows), jnp.float32)
        for b in range(n_sp):
            raw += lax.dot_general(
                w_rope[:, b * depth : (b + 1) * depth],
                normed[b],
                (((1,), (1,)), ((), ())),
                preferred_element_type=jnp.float32,
            )
        half = ROPE // 2
        index = lax.broadcasted_iota(jnp.int32, (half, rows), 1)
        channel = lax.broadcasted_iota(jnp.int32, (half, rows), 0)
        inverse = jnp.zeros((half, rows), jnp.float32)
        for c, value in enumerate(frequency):
            inverse = jnp.where(channel == c, value, inverse)
        values = []
        for i in range(prompts):
            position = offsets[i] + z * rows + index
            angle = position.astype(jnp.float32) * inverse
            sine, cosine = jnp.sin(angle), jnp.cos(angle)
            first = raw[:half, i * rows : (i + 1) * rows]
            second = raw[half:, i * rows : (i + 1) * rows]
            turned = [first * cosine - second * sine, second * cosine + first * sine]
            values.append(jnp.concatenate(turned, axis=0).astype(jnp.bfloat16))
        finalize(0, values)

    def group_item(g):
        value = acc[g][...].astype(jnp.bfloat16)
        finalize(g + 1, [value[i * rows : (i + 1) * rows] for i in range(prompts)])

    def latent_item(m):
        if m == 0:
            rope_item()
        else:
            group_item(m - 1)
        stage_l(m)

    stages = {
        "own": own_z,
        "norm": norm_piece,
        "odot": own_dot,
        "z": stage_z,
        "a": stage_a,
        "b": stage_b,
        "c": stage_c,
        "dot": stage_dot,
        "l": latent_item,
        "t": stage_t,
        "d": stage_d,
        "e": stage_e,
        "end": stage_end,
    }

    def run(schedule, middle):
        finish.clear()
        fetched.clear()
        for name, *args in schedule:
            if name == "a" and not middle:
                stage_z(*args)
            stages[name](*args)
            while len(finish) > PENDING:
                finish.pop(0)()
        for fn in finish:
            fn()

    if tuned:
        inner = has_up & has_down
        pl.when(inner)(lambda: run(MIDDLE, True))
        pl.when(jnp.logical_not(inner))(lambda: run(OUTER, False))
    else:
        run(plain_schedule(units, groups, n_sp), False)


def gather_latent(tokens, w_latent, w_rope, in_gain, offsets, frequency):
    prompts, rows, width = tokens.shape
    n_grp, n_sp, n_tp = (lax.axis_size(a) for a in ("grp", "sp", "tp"))
    n_x = n_tp // CORES
    depth, cols = w_latent.shape
    spans = column_groups(n_sp, cols)
    groups = len(spans)
    chunk = depth // (n_grp * n_tp)
    total = prompts * rows
    units = groups * (n_sp - 1)
    peers = max(n_x, n_grp) - 1
    others = max(n_x - 1, 1)
    items = groups + 1
    bf16, f32 = jnp.bfloat16, jnp.float32
    dma = pltpu.SemaphoreType.DMA
    stay = lambda a: pltpu.with_memory_space_constraint(a, pltpu.HBM)
    limit = (40 if groups > 1 else 60) * 1024 * 1024
    vmem = pl.BlockSpec(memory_space=pltpu.VMEM)
    hbm = pl.BlockSpec(memory_space=pltpu.HBM)
    return pl.pallas_call(
        functools.partial(gather_kernel, n_grp, n_sp, n_tp, spans, frequency),
        out_shape=(
            jax.ShapeDtypeStruct((n_sp, rows, cols), bf16),
            jax.ShapeDtypeStruct((n_sp, ROPE, rows), bf16),
        ),
        in_specs=[hbm, hbm, hbm, hbm, pl.BlockSpec(memory_space=pltpu.SMEM)],
        out_specs=(vmem, vmem),
        scratch_shapes=[
            pltpu.VMEM((total, width), bf16),
            pltpu.VMEM((depth, cols), bf16),
            pltpu.VMEM((ROPE, width), bf16),
            pltpu.VMEM((1, width), f32),
            pltpu.VMEM((n_sp, total, depth), bf16),
            *[pltpu.VMEM((n_sp, CORES, n_x, n_grp, chunk, w), bf16) for _, w in spans],
            *[pltpu.VMEM((total, w), f32) for _, w in spans],
            *[pltpu.VMEM((prompts, rows, w), bf16) for _, w in spans],
            *[pltpu.VMEM((others, prompts, rows, w), bf16) for _, w in spans],
            pltpu.VMEM((prompts, ROPE, rows), bf16),
            pltpu.VMEM((others, prompts, ROPE, rows), bf16),
            dma((4,)),
            dma((groups, 2, 2)),
            dma((units, 2)),
            dma((groups, n_sp, 2)),
            dma((units, peers)),
            dma((units, peers)),
            dma((units, peers)),
            dma((units, peers)),
            dma((units,)),
            dma((units,)),
            dma((items, prompts)),
            dma((items, others, prompts)),
            dma((items, others, prompts)),
            dma((items, prompts, others)),
            dma((items, n_sp, others)),
            dma((items, n_sp)),
            dma((items, n_sp)),
        ],
        compiler_params=pltpu.CompilerParams(
            collective_id=0, has_side_effects=True, vmem_limit_bytes=limit
        ),
    )(*map(stay, (tokens.reshape(total, width), w_latent, w_rope, in_gain)), offsets)


def cache_kernel(
    latent_ref,
    gain_ref,
    wk_ref,
    wv_ref,
    q_nope_ref,
    q_rope_ref,
    rope_ref,
    keys_hbm,
    values_hbm,
    rope_keys_ref,
    read_ref,
    latents,
    keys,
    values,
    sems,
):
    n_blocks, rows, out_cols = keys.shape
    heads = out_cols // HEAD

    def per_head(row, size):
        wide = jnp.broadcast_to(row.astype(jnp.float32), (heads, heads * size))
        head = lax.broadcasted_iota(jnp.int32, wide.shape, 0)
        lane = lax.broadcasted_iota(jnp.int32, wide.shape, 1)
        return jnp.where((lane >= head * size) & (lane < head * size + size), wide, 0.0)

    def put(b, source, target, kind):
        copy = pltpu.make_async_copy(
            source.at[b], target.at[pl.ds(b * rows, rows), :], sems.at[kind, b]
        )
        copy.start()
        return copy

    query = per_head(q_nope_ref[...], HEAD).astype(jnp.bfloat16)
    spread = (heads * ROPE, ROPE)
    fold = lax.broadcasted_iota(jnp.int32, spread, 0) % ROPE == lax.broadcasted_iota(
        jnp.int32, spread, 1
    )
    rotary_q = jnp.dot(
        per_head(q_rope_ref[...], ROPE).astype(jnp.bfloat16),
        jnp.where(fold, 1.0, 0.0).astype(jnp.bfloat16),
        preferred_element_type=jnp.float32,
    ).astype(jnp.bfloat16)
    across = (((1,), (1,)), ((), ()))
    copies, scores = [], []

    def normalize(b):
        raw = latent_ref[b].astype(jnp.float32)
        scale = lax.rsqrt(jnp.mean(raw * raw, axis=-1, keepdims=True) + EPS)
        latents[b] = (raw * scale * gain_ref[...]).astype(jnp.bfloat16)

    def up_key(b):
        block = jnp.dot(latents[b], wk_ref[...], preferred_element_type=jnp.float32)
        keys[b] = block.astype(jnp.bfloat16)
        copies.append(put(b, keys, keys_hbm, 0))

    def up_value(b):
        block = jnp.dot(latents[b], wv_ref[...], preferred_element_type=jnp.float32)
        values[b] = block.astype(jnp.bfloat16)
        copies.append(put(b, values, values_hbm, 1))

    def score(b):
        part = lax.dot_general(query, keys[b], across, preferred_element_type=jnp.float32)
        part += jnp.dot(rotary_q, rope_ref[b], preferred_element_type=jnp.float32)
        scores.append(part / jnp.sqrt(jnp.float32(HEAD + ROPE)))
        rope_keys_ref[:, b * rows : (b + 1) * rows] = rope_ref[b]

    normalize(0)
    for b in range(n_blocks):
        if b + 1 < n_blocks:
            normalize(b + 1)
        up_key(b)
        if b + 1 < n_blocks:
            up_value(b)
        score(b)
    up_value(n_blocks - 1)
    peak = functools.reduce(jnp.maximum, scores).max(axis=-1, keepdims=True)
    expos = [jnp.exp(part - peak) for part in scores]
    total = functools.reduce(jnp.add, expos).sum(axis=-1, keepdims=True)
    out = jnp.zeros((heads, out_cols), jnp.float32)
    for b in range(n_blocks):
        weights = (expos[b] / total).astype(jnp.bfloat16)
        out += jnp.dot(weights, values[b], preferred_element_type=jnp.float32)
    head = lax.broadcasted_iota(jnp.int32, out.shape, 0)
    lane = lax.broadcasted_iota(jnp.int32, out.shape, 1)
    picked = jnp.where((lane >= head * HEAD) & (lane < head * HEAD + HEAD), out, 0.0)
    read_ref[...] = jnp.sum(picked, axis=0, keepdims=True).astype(jnp.bfloat16)
    for copy in copies:
        copy.wait()


def fill_cache(latent, kv_gain, w_up_key, w_up_value, q_nope, q_rope, rope):
    n_blocks, rows, cols = latent.shape
    out_cols = w_up_key.shape[1]
    length = n_blocks * rows
    vmem = pl.BlockSpec(memory_space=pltpu.VMEM)
    hbm = pl.BlockSpec(memory_space=pltpu.HBM)
    return pl.pallas_call(
        cache_kernel,
        out_shape=(
            jax.ShapeDtypeStruct((length, out_cols), jnp.bfloat16),
            jax.ShapeDtypeStruct((length, out_cols), jnp.bfloat16),
            jax.ShapeDtypeStruct((ROPE, length), jnp.bfloat16),
            jax.ShapeDtypeStruct((1, out_cols), jnp.bfloat16),
        ),
        in_specs=[vmem] * 7,
        out_specs=(hbm, hbm, vmem, vmem),
        scratch_shapes=[
            pltpu.VMEM((n_blocks, rows, cols), jnp.bfloat16),
            pltpu.VMEM((n_blocks, rows, out_cols), jnp.bfloat16),
            pltpu.VMEM((n_blocks, rows, out_cols), jnp.bfloat16),
            pltpu.SemaphoreType.DMA((2, n_blocks)),
        ],
        compiler_params=pltpu.CompilerParams(vmem_limit_bytes=40 * 1024 * 1024),
    )(latent, kv_gain, w_up_key, w_up_value, q_nope, q_rope, rope)


def local(
    tokens, offsets, in_gain, w_latent, w_rope_key, kv_gain, w_up_key, w_up_value, q_nope, q_rope
):
    steps = -np.arange(0, ROPE, 2).astype(np.float32) / ROPE
    frequency = [float(f) for f in np.float32(10000.0) ** steps]
    latent, rope = gather_latent(tokens, w_latent, w_rope_key.T, in_gain[None], offsets, frequency)
    keys, values, rope_keys, read = fill_cache(
        latent, kv_gain[None], w_up_key, w_up_value, q_nope, q_rope, rope
    )
    return (keys[None], values[None], rope_keys[None], read)


def solution(mesh):
    in_specs = (
        P(("grp", "tp"), "sp", None),
        P(("grp", "tp")),
        P(),
        P("sp", None),
        P(),
        P(),
        P(None, "tp"),
        P(None, "tp"),
        P(("grp", "sp"), "tp"),
        P(("grp", "sp"), "tp"),
    )
    out_specs = (
        P(("grp", "sp"), None, "tp"),
        P(("grp", "sp"), None, "tp"),
        P(("grp", "sp"), None, None),
        P(("grp", "sp"), "tp"),
    )
    return jax.shard_map(local, mesh=mesh, in_specs=in_specs, out_specs=out_specs, check_vma=False)
```
